256 devices in a mesh: sp: 64 (over z, x, core), tp: 4 (over y).
Axes of the slice: x: 4, y: 4, z: 8, core: 2. Of those that a mesh axis runs over, the one named last changes fastest.
Arguments:
- residual_in: bfloat16 [16384, 2048], P(('sp', 'tp')), may hold values from -6 to 6
- queries: bfloat16 [16384, 512], P('sp', 'tp'), may hold values from -6 to 6
- key_rows: bfloat16 [16384, 512], P('sp', 'tp'), may hold values from -6 to 6
- value_rows: bfloat16 [16384, 1024], P('sp', 'tp'), may hold values from -6 to 6
- out_gate: bfloat16 [16384, 1024], P('sp', 'tp'), may hold values from -6 to 6
- decay_logit: float32 [16384, 512], P('sp', 'tp'), may hold values from -30 to 30
- head_gain: bfloat16 [128], replicated, may hold values from 0.099609375 to 1.8984375
- w_out: bfloat16 [1024, 2048], replicated, may hold values from -0.1875 to 0.1875
- ffn_gain: bfloat16 [2048], replicated, may hold values from 0.099609375 to 1.8984375
- routing: int32 [16384, 4], P('sp'), may hold values from 0 to 63, all different within a row; in each aligned block of 64 rows (0 to 63, 64 to 127, ...) at most 8 rows name the same one
- route_weight: float32 [16384, 4], P(('sp', 'tp')), may hold values from 0.05 to 0.6
- w_gate: bfloat16 [64, 2048, 2048], P('sp', None, 'tp'), may hold values from -4 to 4
- w_up: bfloat16 [64, 2048, 2048], P('sp', None, 'tp'), may hold values from -4 to 4
- w_down: bfloat16 [64, 2048, 2048], P('sp', 'tp'), may hold values from -0.125 to 0.125
Outputs:
- layer_out: bfloat16 [16384, 2048], P(('sp', 'tp'))
The draws below stay inside these ranges and needn't reach their ends.
Inputs may be any that keep to these rules, and one draw needn't show every extreme that they name: `routing`: each row names 4 different experts. In each aligned block of 64 rows no expert is named more than 8 times, a bound that some blocks reach.
All inputs are finite; a program needn't handle non-finite values.
Results may differ from the reference program's by a relative error of at most 0.03.
Values may be sent and summed in bfloat16 or wider, within the bound.
No kernel may reach another device: no remote copies, remote signals or barrier semaphores. Data moves between devices by JAX's collectives and lax.ppermute only.
A program may use at most 128 MiB of HBM per device.

```python
import math
import jax
import jax.numpy as jnp
import numpy as np
from jax import lax

D = 2048
HEADS = 8
DK = 64
DV = 128
FF = 2048
TOP = 4
BLOCK = 64
TOK_DEV = 256
TOKEN_COUNT = 16384
EXPERTS = 64
QROWS = 64
CAP = 8
N_TP = 4


def draw_decay_logit(key, part):
    random_subkeys = jax.random.split(jax.random.fold_in(key, 31), 7)
    channels = HEADS * DK
    share_fast = 0.5
    fast_head = jax.random.uniform(random_subkeys[0], (HEADS,)) < share_fast
    fast_channel = jnp.repeat(fast_head, DK)
    fast_rate = jnp.exp(jax.random.uniform(random_subkeys[1], (channels,), minval=jnp.log(1.0 / 50.0), maxval=jnp.log(1.0 / 15.0)))
    slow_rate = jnp.exp(jax.random.uniform(random_subkeys[2], (channels,), minval=jnp.log(0.3), maxval=0.0)) * 0.7 / TOKEN_COUNT
    base_rate = jnp.where(fast_channel, fast_rate, slow_rate)
    span_count = TOKEN_COUNT // TOK_DEV
    span_factor = jnp.repeat(jnp.exp(jax.random.uniform(random_subkeys[3], (span_count,), minval=jnp.log(0.5), maxval=jnp.log(2.0))), TOK_DEV)
    jitter = jnp.exp(0.6 * jax.random.truncated_normal(random_subkeys[4], -3.0, 3.0, (TOKEN_COUNT, channels)))
    stepwise_results = base_rate[None, :] * span_factor[:, None] * jitter
    spike_location = jax.random.randint(random_subkeys[5], (3,), 0, TOKEN_COUNT)
    spike_penalty = jax.random.uniform(random_subkeys[6], (3,), minval=0.2, maxval=0.45)
    position_indices = jnp.arange(TOKEN_COUNT)
    spike_increment = jnp.sum(jnp.where(position_indices[:, None] == spike_location[None, :], -jnp.log(1.0 - spike_penalty)[None, :], 0.0), axis=1)
    stepwise_results = stepwise_results + spike_increment[:, None]
    scaled = 16.0 * stepwise_results
    return -jnp.log(jnp.expm1(scaled))


def column_scaled(key, salt_value):
    random_subkeys = jax.random.split(jax.random.fold_in(key, salt_value), 2)
    lowest = 0.3
    highest = 2.5
    scales = jnp.exp(jax.random.uniform(random_subkeys[0], (EXPERTS, 1, FF), minval=jnp.log(lowest), maxval=jnp.log(highest)))
    entries = jax.random.truncated_normal(random_subkeys[1], -4.0, 4.0, (EXPERTS, D, FF))
    return entries * scales * D ** (-0.5)


def draw_w_gate(key, part):
    return column_scaled(key, 11).astype(jnp.bfloat16)


def draw_w_up(key, part):
    return column_scaled(key, 12).astype(jnp.bfloat16)


def block_levels(rng, shape, pieces, least, top_value):
    level = 1.0
    for dim, shards_of in pieces:
        draws = jax.random.uniform(jax.random.fold_in(jax.random.fold_in(rng, 6), dim), (shards_of,), jnp.float32, least / len(pieces), top_value / len(pieces))
        level = level * jnp.repeat(jnp.exp(draws), shape[dim] // shards_of).reshape((-1,) + (1,) * (len(shape) - 1 - dim))
    return level


def deal_out(rng, own, number, rows, number_of, top, limit, skew):
    sequence = jax.random.permutation(rng, number_of)
    crowded, ordinary = shares(number_of, rows * top, limit, skew, True), shares(number_of, rows * top, limit, skew, False)
    places = jnp.arange(number_of)

    def named(tallies, turn):
        used = int((tallies > 0).sum())
        fixed = max(1, used // 4)
        shifted = fixed + (places - fixed + turn * (used - fixed)) % max(1, number_of - fixed)
        return jnp.zeros((number_of,), jnp.int32).at[sequence[jnp.where(places < fixed, places, shifted)]].set(jnp.asarray(tallies, jnp.int32))

    tallies = jnp.where(number % 4 == 0, named(crowded, number // 4), named(ordinary, number - number // 4 - 1))
    mixed = jax.random.permutation(jax.random.fold_in(own, 3), number_of)
    source_of, receiver = mixed[0:number_of // 2 * 2:2], mixed[1:number_of // 2 * 2:2]
    margin = jnp.minimum(tallies[source_of] - 1, limit - tallies[receiver]) // 2
    margin = jnp.where((source_of == sequence[0]) | (receiver == sequence[0]) | (tallies[receiver] == 0), 0, jnp.maximum(margin, 0))
    shifted = jax.random.randint(jax.random.fold_in(own, 4), (number_of // 2,), 0, 1 << 20) % (margin + 1)
    tallies = tallies.at[source_of].add(-shifted).at[receiver].add(shifted)
    items = jnp.searchsorted(jnp.cumsum(tallies), jnp.arange(rows * top), side="right").astype(jnp.int32)
    listing = items.reshape(top, rows).T
    listing = listing[jax.random.permutation(jax.random.fold_in(own, 1), rows)]
    turn = jax.random.randint(jax.random.fold_in(own, 2), (rows, 1), 0, top)
    return jnp.take_along_axis(listing, (jnp.arange(top)[None, :] + turn) % top, axis=1)


def shares(amount, total, reach, skew, full):
    weights = [(1 << 20) // math.isqrt(rank ** skew) + 1 for rank in range(1, amount + 1)]
    largest = reach if full else min(reach, max(-(-total // amount), total * weights[0] // sum(weights)))
    least = 1 if total - largest >= amount - 1 else 0
    counts, surplus = [largest] + [least] * (amount - 1), total - largest - least * (amount - 1)
    while surplus > 0:
        free = [i for i in range(1, amount) if counts[i] < largest] or [i for i in range(1, amount) if counts[i] < reach]
        whole, left = sum([weights[i] for i in free]), surplus
        for i in free:
            more = min(reach - counts[i], max(1, left * weights[i] // whole), surplus)
            counts[i] = counts[i] + more
            surplus = surplus - more
    return np.array(counts)


def normal_values(rng, extent, scale, bound, cuts=(), held_as=jnp.bfloat16):
    values = scale * jax.random.normal(rng, extent, jnp.float32)
    if cuts:
        values = values * block_levels(rng, extent, cuts, -0.22, 0.18)
    return jnp.clip(values, -bound, bound).astype(held_as)


def setup_inputs(seed: int = 0) -> dict:
    arg_keys = jax.random.split(jax.random.key(seed), 15)
    residual_in = normal_values(arg_keys[0], (TOKEN_COUNT, D), 1.0, 6.0, ((0, 256),))
    queries = normal_values(arg_keys[1], (TOKEN_COUNT, HEADS * DK), 1.0, 6.0, ((0, 64), (1, 4)))
    key_rows = normal_values(arg_keys[2], (TOKEN_COUNT, HEADS * DK), 1.0, 6.0, ((0, 64), (1, 4)))
    value_rows = normal_values(arg_keys[3], (TOKEN_COUNT, HEADS * DV), 1.0, 6.0, ((0, 64), (1, 4)))
    out_gate = normal_values(arg_keys[4], (TOKEN_COUNT, HEADS * DV), 1.0, 6.0, ((0, 64), (1, 4)))
    decay_logit = draw_decay_logit(jax.random.fold_in(arg_keys[14], 71), 0)
    head_gain = jnp.clip(1.0 + 0.18 * jax.random.normal(arg_keys[6], (DV,), jnp.float32), 0.099609375, 1.8984375).astype(jnp.bfloat16)
    w_out = normal_values(arg_keys[7], (HEADS * DV, D), (HEADS * DV) ** -0.5, 0.1875)
    ffn_gain = jnp.clip(1.0 + 0.18 * jax.random.normal(arg_keys[8], (D,), jnp.float32), 0.099609375, 1.8984375).astype(jnp.bfloat16)
    routing_keys = jax.random.split(jax.random.fold_in(arg_keys[9], 1), TOKEN_COUNT // QROWS)
    routing_turns = jax.random.permutation(jax.random.fold_in(arg_keys[9], 3), TOKEN_COUNT // QROWS)
    routing = jax.vmap(lambda own, number: deal_out(jax.random.fold_in(arg_keys[9], 2), own, number, QROWS, EXPERTS, TOP, CAP, 2))(routing_keys, routing_turns).reshape((TOKEN_COUNT, TOP))
    route_weight = jnp.clip(jnp.exp(math.log(0.6) - 2.4849067 * jax.random.uniform(arg_keys[10], (TOKEN_COUNT, TOP), jnp.float32) ** block_levels(arg_keys[10], (TOKEN_COUNT, TOP), ((0, 256),), -0.2, 0.2)), 0.05, 0.6)
    w_gate = draw_w_gate(jax.random.fold_in(arg_keys[14], 71), 0)
    w_up = draw_w_up(jax.random.fold_in(arg_keys[14], 71), 0)
    w_down = normal_values(arg_keys[13], (EXPERTS, FF, D), FF ** -0.5, 0.125, ((0, 64), (1, 4)))
    return dict(residual_in=residual_in, queries=queries, key_rows=key_rows, value_rows=value_rows, out_gate=out_gate, decay_logit=decay_logit, head_gain=head_gain, w_out=w_out, ffn_gain=ffn_gain, routing=routing, route_weight=route_weight, w_gate=w_gate, w_up=w_up, w_down=w_down)


DECAY_TEMP = 16.0
CLAMP_LIMIT = 7.0
SIGMOID_SLOPE = 1.702
NORM_EPS = 1e-06
EXACT_PRECISION = lax.Precision.HIGHEST

def block_parts(query_blk, key_blk, value_blk, logdecay_blk):
    cumulative = jnp.cumsum(logdecay_blk, axis=2)
    length = cumulative.shape[2]
    causal = (jnp.arange(length)[:, None] >= jnp.arange(length)[None, :])[:, :, None]
    spread = cumulative[:, :, :, None, :] - cumulative[:, :, None, :, :]
    weighted = query_blk[:, :, :, None, :] * jnp.exp(jnp.where(causal, spread, -jnp.inf))
    scores = jnp.einsum('nhtsk,nhsk->nhts', weighted, key_blk, precision=EXACT_PRECISION)
    inner_part = jnp.einsum('nhts,nhsv->nhtv', scores, value_blk, precision=EXACT_PRECISION)
    ending = cumulative[:, :, -1:, :]
    contrib = jnp.einsum('nhsk,nhsv->nhkv', key_blk * jnp.exp(ending - cumulative), value_blk, precision=EXACT_PRECISION)
    return (inner_part, query_blk * jnp.exp(cumulative), contrib, jnp.exp(ending[:, :, 0, :]))

def carry_blocks(query_dec, contrib, passing, begin):

    def advance(recurrent_state, inputs):
        current_query, contrib_now, passing_now = inputs
        state_readout = jnp.einsum('uaz,uze->uae', current_query, recurrent_state, precision=EXACT_PRECISION)
        return (passing_now[..., None] * recurrent_state + contrib_now, state_readout)
    final_state, readouts = lax.scan(advance, begin, (query_dec, contrib, passing))
    return (readouts, final_state)

def finish_heads(blocks_out, head_gain, out_gate):
    count_blk, head_count, length, head_width = blocks_out.shape
    tokens = count_blk * length
    attended = blocks_out.transpose(0, 2, 1, 3).reshape(tokens, head_count, head_width)
    inv_scale = lax.rsqrt(lax.optimization_barrier(jnp.mean(attended * attended, axis=-1, keepdims=True)) + NORM_EPS)
    headed = attended * inv_scale * head_gain.astype(jnp.float32)
    gated = headed.reshape(tokens, head_count * head_width) * jax.nn.silu(out_gate.astype(jnp.float32))
    return gated.astype(jnp.bfloat16)

def norm_rows(residual, gain_vec):
    values = residual.astype(jnp.float32)
    inv_scale = lax.rsqrt(lax.optimization_barrier(jnp.mean(values * values, axis=-1, keepdims=True)) + NORM_EPS)
    return (values * inv_scale * gain_vec.astype(jnp.float32)).astype(jnp.bfloat16)

def clamped_unit(gate_pre, up_pre):
    gate_cut = jnp.minimum(gate_pre, CLAMP_LIMIT)
    up_cut = jnp.clip(up_pre, -CLAMP_LIMIT, CLAMP_LIMIT)
    return (up_cut + 1.0) * (gate_cut * jax.nn.sigmoid(SIGMOID_SLOPE * gate_cut))

def slot_ids(routes, capacity, experts):
    batch_size, rows_each, top_count = routes.shape
    flat_ids = routes.reshape(batch_size, rows_each * top_count)
    onehot = (flat_ids[:, :, None] == jnp.arange(experts, dtype=jnp.int32)[None, None, :]).astype(jnp.int32)
    earlier = jnp.cumsum(onehot, axis=1) - onehot
    rank_in = lax.optimization_barrier(jnp.sum(earlier * onehot, axis=2))
    return (flat_ids * capacity + rank_in).reshape(batch_size, rows_each, top_count)

def reference(residual_in, queries, key_rows, value_rows, out_gate, decay_logit, head_gain, w_out, ffn_gain, routing, route_weight, w_gate, w_up, w_down):
    groups = TOKEN_COUNT // TOK_DEV

    def grouped(array, head_width):
        shaped = array.astype(jnp.float32).reshape(groups, TOK_DEV // BLOCK, BLOCK, HEADS, head_width)
        return shaped.transpose(0, 1, 3, 2, 4)
    query_grp = grouped(queries, DK) * DK ** (-0.5)
    key_grp = grouped(key_rows, DK)
    value_grp = grouped(value_rows, DV)
    logdecay_grp = grouped(jax.nn.log_sigmoid(decay_logit) / DECAY_TEMP, DK)

    def through(recurrent_state, inputs):
        current_query, key_now, value_now, decay_now = inputs
        inner_part, query_dec, contrib, passing = block_parts(current_query, key_now, value_now, decay_now)
        readouts, final_state = carry_blocks(query_dec, contrib, passing, recurrent_state)
        return (final_state, inner_part + readouts)
    _, outputs = lax.scan(through, jnp.zeros((HEADS, DK, DV), jnp.float32), (query_grp, key_grp, value_grp, logdecay_grp))
    mixed_out = finish_heads(outputs.reshape(TOKEN_COUNT // BLOCK, HEADS, BLOCK, DV), head_gain, out_gate)
    projected = jnp.dot(mixed_out, w_out, preferred_element_type=jnp.float32)
    residual = (residual_in.astype(jnp.float32) + projected).astype(jnp.bfloat16)
    normed = norm_rows(residual, ffn_gain)
    blocks = TOKEN_COUNT // QROWS
    ranked = slot_ids(routing.reshape(blocks, QROWS, TOP), CAP, EXPERTS).reshape(blocks, QROWS * TOP)
    flat_expert = routing.reshape(blocks, QROWS * TOP)
    rank_in = ranked - flat_expert * CAP
    placed = (flat_expert * (blocks * CAP) + jnp.arange(blocks, dtype=jnp.int32)[:, None] * CAP + rank_in).reshape(-1)
    token_of = jnp.repeat(jnp.arange(TOKEN_COUNT, dtype=jnp.int32), TOP)
    slots_all = EXPERTS * blocks * CAP
    token_table = jnp.zeros((slots_all,), jnp.int32).at[placed].set(token_of).reshape(EXPERTS, blocks * CAP)
    weight_table = jnp.zeros((slots_all,), jnp.float32).at[placed].set(route_weight.reshape(-1)).reshape(EXPERTS, blocks * CAP)
    live_slot = jnp.zeros((slots_all,), jnp.float32).at[placed].set(1.0).reshape(EXPERTS, blocks * CAP)
    part_width = FF // N_TP

    def serve_expert(accumulated, inputs):
        token_ids, slot_weight, slot_live, gate_cols, up_cols, down_rows = inputs
        gathered = jnp.where(slot_live[:, None] > 0, normed[token_ids], jnp.zeros((), jnp.bfloat16))
        gate_pre = jnp.dot(gathered, gate_cols, preferred_element_type=jnp.float32)
        up_pre = jnp.dot(gathered, up_cols, preferred_element_type=jnp.float32)
        hidden = clamped_unit(gate_pre, up_pre).astype(jnp.bfloat16)
        expert_out = jnp.zeros((gathered.shape[0], D), jnp.float32)
        for shard_no in range(N_TP):
            portion = jnp.dot(hidden[:, shard_no * part_width:(shard_no + 1) * part_width], down_rows[shard_no * part_width:(shard_no + 1) * part_width], preferred_element_type=jnp.float32).astype(jnp.bfloat16)
            portion = lax.optimization_barrier(portion)
            expert_out = expert_out + portion.astype(jnp.float32)
        expert_out = expert_out.astype(jnp.bfloat16)
        return (accumulated.at[token_ids].add(slot_weight[:, None] * expert_out.astype(jnp.float32)), None)
    routed, _ = lax.scan(serve_expert, jnp.zeros((TOKEN_COUNT, D), jnp.float32), (token_table, weight_table, live_slot, w_gate, w_up, w_down))
    return (residual.astype(jnp.float32) + routed).astype(jnp.bfloat16)
```

```python
import jax
import jax.numpy as jnp
from jax import lax
from jax.experimental import pallas as pl
from jax.experimental.pallas import tpu as pltpu
from jax.sharding import Mesh
from jax.sharding import PartitionSpec as P


DK = 64
DV = 128
BLOCK = 64
SP = ("sp_0", "sp_1", "sp_2")
SP_TP = ("sp_0", "sp_1", "sp_2", "tp")
PLANE = ("sp_1", "sp_2")
DECAY_TEMP = 16.0
CLAMP_LIMIT = 7.0
SIGMOID_SLOPE = 1.702
NORM_EPS = 1e-06
F32 = jnp.float32
BF16 = jnp.bfloat16

ROW_PAIRS = [(c * 4 + y, c * 4 + ((y ^ 1) if c == 0 else 3 - y)) for c in range(2) for y in range(4)]
WEIGHT_PAIRS = [(c * 4 + y, c * 4 + ((3 - y) if c == 0 else (y ^ 1))) for c in range(2) for y in range(4)]


def dot(a, b, dims):
    return lax.dot_general(a, b, (dims, ((), ())), preferred_element_type=F32)


def split3(x):
    hi = x.astype(BF16)
    rest = x - hi.astype(F32)
    mid = rest.astype(BF16)
    return hi, mid, (rest - mid.astype(F32)).astype(BF16)


def head_mask(shape):
    return lax.broadcasted_iota(jnp.int32, shape, 1) < DK


def pick_heads(both):
    top, bottom = both[:DV], both[DV:]
    return jnp.where(head_mask(top.shape), top, bottom)


def stack_heads(x):
    zero = jnp.zeros_like(x)
    mask = head_mask(x.shape)
    return jnp.concatenate([jnp.where(mask, x, zero), jnp.where(mask, zero, x)], axis=0)


def store_state(out_ref, state_t, log_total):
    packed = jnp.concatenate(
        [
            state_t,
            *(part.astype(F32) for part in split3(log_total)),
            jnp.zeros((5, 2 * DK), F32),
        ],
        axis=0,
    ).astype(BF16)
    for copy in range(out_ref.shape[0]):
        out_ref[copy] = packed


def load_state(ref, k):
    item = ref[k].astype(F32)
    return item[:DV], item[DV : DV + 1] + item[DV + 1 : DV + 2] + item[DV + 2 : DV + 3]


def local_kernel(k_ref, v_ref, d_ref, state_ref, cum_ref):
    logit = d_ref[...]
    logdecay = (jnp.minimum(logit, 0.0) - jnp.log1p(jnp.exp(-jnp.abs(logit)))) / DECAY_TEMP
    rows = logdecay.shape[0]
    low = (
        lax.broadcasted_iota(jnp.int32, (rows, rows), 0)
        >= lax.broadcasted_iota(jnp.int32, (rows, rows), 1)
    ).astype(F32).astype(BF16)
    cum = sum(dot(low, part, ((1,), (0,))) for part in split3(logdecay))
    cum_ref[...] = cum
    end = cum[rows - 1 : rows]
    kdec = (k_ref[...].astype(F32) * jnp.exp(end - cum)).astype(BF16)
    state_t = pick_heads(dot(v_ref[...], kdec, ((0,), (0,))))
    store_state(state_ref, state_t, end)


def inner_kernel(q_ref, k_ref, v_ref, cum_ref, inner_ref, qdec_ref):
    rows = q_ref.shape[0]
    half = BLOCK // 2
    cum_all = cum_ref[...]
    q_all = q_ref[...].astype(F32) * (DK**-0.5)
    qdec_ref[...] = (q_all * jnp.exp(cum_all)).astype(BF16)
    row = lax.broadcasted_iota(jnp.int32, (BLOCK, 2 * DK), 0)
    t = lax.broadcasted_iota(jnp.int32, (2 * BLOCK, BLOCK), 0) % BLOCK
    s = lax.broadcasted_iota(jnp.int32, (2 * BLOCK, BLOCK), 1)
    near = (t >= s) & ((t < half) == (s < half))
    far = (t >= half) & (s < half)
    state = jnp.zeros((DV, 2 * DK), F32)
    for b in range(rows // BLOCK):
        at = slice(b * BLOCK, (b + 1) * BLOCK)
        cum = cum_all[at]
        if b:
            cum = cum - cum_all[b * BLOCK - 1 : b * BLOCK]
        q, k, v = q_all[at], k_ref[at, :].astype(F32), v_ref[at, :]
        middle = jnp.where(row < half, cum[half // 2 - 1 : half // 2], cum[half + half // 2 - 1 : half + half // 2])
        border = cum[half - 1 : half]
        end = cum[BLOCK - 1 : BLOCK]
        shifted = cum - middle
        q_near = (q * jnp.exp(shifted)).astype(BF16)
        k_near = (k * jnp.exp(-shifted)).astype(BF16)
        q_far = (q * jnp.exp(jnp.minimum(cum - border, 0.0))).astype(BF16)
        k_far = (k * jnp.exp(jnp.minimum(border - cum, 0.0))).astype(BF16)
        s_near = dot(stack_heads(q_near), k_near, ((1,), (1,)))
        s_far = dot(stack_heads(q_far), k_far, ((1,), (1,)))
        scores = jnp.where(near, s_near, jnp.where(far, s_far, 0.0)).astype(BF16)
        part0 = dot(scores[:BLOCK], v[:, :DV], ((1,), (0,)))
        part1 = dot(scores[BLOCK:], v[:, DV:], ((1,), (0,)))
        if b:
            read = dot(stack_heads((q * jnp.exp(cum)).astype(BF16)), state.astype(BF16), ((1,), (1,)))
            part0 = part0 + read[:BLOCK]
            part1 = part1 + read[BLOCK:]
        inner_ref[at, :DV] = part0
        inner_ref[at, DV:] = part1
        if (b + 1) * BLOCK < rows:
            kdec = (k * jnp.exp(end - cum)).astype(BF16)
            added = pick_heads(dot(v, kdec, ((0,), (0,))))
            state = added if b == 0 else state * jnp.exp(end) + added


def plane_kernel(at_ref, all_ref, total_ref, before_ref, logb_ref):
    place = at_ref[0]
    before = total = jnp.zeros((DV, 2 * DK), F32)
    log_before = log_total = jnp.zeros((1, 2 * DK), F32)
    for k in range(all_ref.shape[0]):
        state, log = load_state(all_ref, k)
        decay = jnp.exp(log)
        total = total * decay + state
        log_total = log_total + log
        before = jnp.where(k < place, before * decay + state, before)
        log_before = jnp.where(k < place, log_before + log, log_before)
    store_state(total_ref, total, log_total)
    before_ref[...] = before
    logb_ref[...] = jnp.broadcast_to(log_before, logb_ref.shape)


def finish_kernel(at_ref, all_ref, before_ref, logb_ref, inner_ref, qdec_ref, gate_ref, gain_ref, out_ref):
    place = at_ref[0]
    state = jnp.zeros((DV, 2 * DK), F32)
    for k in range(all_ref.shape[0]):
        added, log = load_state(all_ref, k)
        state = jnp.where(k < place, state * jnp.exp(log) + added, state)
    state = state * jnp.exp(logb_ref[0:1]) + before_ref[...]
    read = dot(stack_heads(qdec_ref[...]), state.astype(BF16), ((1,), (1,)))
    rows = inner_ref.shape[0]
    quarter = rows // out_ref.shape[0]
    gain = gain_ref[...].astype(F32)
    for h in range(2):
        cols = slice(h * DV, (h + 1) * DV)
        attended = inner_ref[:, cols] + read[h * rows : (h + 1) * rows]
        scale = lax.rsqrt(jnp.mean(attended * attended, axis=1, keepdims=True) + NORM_EPS)
        gate = gate_ref[:, cols].astype(F32)
        mixed = (attended * scale * gain * (gate / (1.0 + jnp.exp(-gate)))).astype(BF16)
        for j in range(out_ref.shape[0]):
            out_ref[j, :, cols] = mixed[j * quarter : (j + 1) * quarter]


def call(kernel, outs, *args, flops=2**20):
    specs = [
        pl.BlockSpec(memory_space=pltpu.SMEM if a.dtype == jnp.int32 else pltpu.VMEM) for a in args
    ]
    return pl.pallas_call(
        kernel,
        out_shape=outs,
        in_specs=specs,
        out_specs=[pl.BlockSpec(memory_space=pltpu.VMEM)] * len(outs),
        cost_estimate=pl.CostEstimate(flops=flops, bytes_accessed=2**19, transcendentals=2**16),
    )(*args)


def shaped(shape, dtype):
    return jax.ShapeDtypeStruct(shape, dtype)


def mixer(queries, key_rows, value_rows, out_gate, decay_logit, head_gain):
    rows = queries.shape[0]
    planes, members, tps = lax.axis_size("sp_0"), lax.axis_size(PLANE), lax.axis_size("tp")
    packed = DV + 8
    state, cum = call(
        local_kernel,
        [shaped((members, packed, 2 * DK), BF16), shaped((rows, 2 * DK), F32)],
        key_rows, value_rows, decay_logit,
    )
    inner, qdec = call(
        inner_kernel,
        [shaped((rows, 2 * DV), F32), shaped((rows, 2 * DK), BF16)],
        queries, key_rows, value_rows, cum,
    )
    in_plane = lax.all_to_all(state, PLANE, 0, 0, tiled=True)
    total, before, logb = call(
        plane_kernel,
        [shaped((planes, packed, 2 * DK), BF16), shaped((DV, 2 * DK), F32), shaped((8, 2 * DK), F32)],
        lax.axis_index(PLANE)[None].astype(jnp.int32), in_plane,
    )
    along = lax.all_to_all(total, "sp_0", 0, 0, tiled=True)
    (mixed,) = call(
        finish_kernel,
        [shaped((tps, rows // tps, 2 * DV), BF16)],
        lax.axis_index("sp_0")[None].astype(jnp.int32), along, before, logb, inner, qdec, out_gate,
        head_gain[None],
    )
    return lax.all_to_all(mixed, "tp", 0, 0, tiled=True)


def clamped_unit(gate_pre, up_pre):
    gate_cut = jnp.minimum(gate_pre, CLAMP_LIMIT)
    up_cut = jnp.clip(up_pre, -CLAMP_LIMIT, CLAMP_LIMIT)
    return (up_cut + 1.0) * (gate_cut / (1.0 + jnp.exp(-SIGMOID_SLOPE * gate_cut)))


def ffn_kernel(x_ref, g0, u0, d0, g1, u1, d1, out_ref, g_buf, u_buf, d_buf, sem):
    copies = [
        [
            pltpu.make_async_copy(src, buf.at[half], sem.at[half, j])
            for j, (src, buf) in enumerate(zip(srcs, (g_buf, u_buf, d_buf)))
        ]
        for half, srcs in enumerate(((g0, u0, d0), (g1, u1, d1)))
    ]
    for half in copies:
        for copy in half:
            copy.start()
    total = None
    for half, (gate_copy, up_copy, down_copy) in enumerate(copies):
        gate_copy.wait()
        gate_pre = dot(x_ref[...], g_buf[half], ((1,), (0,)))
        up_copy.wait()
        up_pre = dot(x_ref[...], u_buf[half], ((1,), (0,)))
        hidden = clamped_unit(gate_pre, up_pre).astype(BF16)
        down_copy.wait()
        part = dot(hidden, d_buf[half], ((1,), (0,)))
        total = part if total is None else total + part
    out_ref[...] = total.astype(out_ref.dtype)


def ffn(x, own, other, dtype):
    rows, width = x.shape
    units = own[0].shape[1]
    return pl.pallas_call(
        ffn_kernel,
        out_shape=shaped((rows, width), dtype),
        in_specs=[pl.BlockSpec(memory_space=pltpu.VMEM)] + [pl.BlockSpec(memory_space=pl.ANY)] * 6,
        out_specs=pl.BlockSpec(memory_space=pltpu.VMEM),
        scratch_shapes=[
            pltpu.VMEM((2, width, units), BF16),
            pltpu.VMEM((2, width, units), BF16),
            pltpu.VMEM((2, units, width), BF16),
            pltpu.SemaphoreType.DMA((2, 3)),
        ],
        cost_estimate=pl.CostEstimate(
            flops=12 * rows * width * units, bytes_accessed=12 * width * units, transcendentals=2 * rows * units
        ),
    )(x, *own, *other)


def blend(rank, weight, cap):
    slots = jnp.arange(cap).astype(F32)
    full = jnp.where(rank[:, :, None] == slots, weight[:, :, None], 0.0).reshape(rank.shape[0], -1)
    lead = lax.reduce_precision(full, 8, 7)
    return lead.astype(BF16), (full - lead).astype(BF16)


def on_device(
    residual_in, queries, key_rows, value_rows, out_gate, decay_logit, head_gain, w_out, ffn_gain,
    routing, route_weight, w_gate, w_up, w_down,
):
    core_tp = ("sp_2", "tp")
    own = (w_gate[0], w_up[0], w_down[0])
    other = []
    for w in own:
        other.append(lax.ppermute(w, core_tp, WEIGHT_PAIRS))
    experts, cores = lax.axis_size(SP), lax.axis_size("sp_2")
    columns = experts // cores
    quarter, width = residual_in.shape
    cap = 2 * routing.shape[0] * routing.shape[1] // (lax.axis_size("tp") * experts)
    slots = jnp.arange(cap).astype(F32)
    swap_cores = [(0, 1), (1, 0)]

    routes = lax.dynamic_slice_in_dim(routing, lax.axis_index("tp") * quarter, quarter, 0)
    named = routes[:, :, None] == jnp.arange(experts, dtype=jnp.int32)
    chosen = jnp.any(named, axis=1)
    weight = jnp.sum(jnp.where(named, route_weight[:, :, None], 0.0), axis=1)
    earlier = jnp.tril(jnp.ones((quarter, quarter), BF16), -1)
    rank = jnp.where(chosen, jnp.dot(earlier, chosen.astype(BF16), preferred_element_type=F32), -1.0)
    both = jnp.stack([rank, weight]).reshape(2, quarter, columns, cores)
    core = lax.axis_index("sp_2")
    here = lax.dynamic_index_in_dim(both, core, 3, keepdims=False)
    away = lax.dynamic_index_in_dim(both, 1 - core, 3, keepdims=False)
    theirs_plan = lax.ppermute(away, "sp_2", swap_cores)
    plans = (here, theirs_plan)

    by_token = mixer(queries, key_rows, value_rows, out_gate, decay_logit, head_gain)
    by_token = by_token.transpose(1, 0, 2).reshape(quarter, -1)
    projected = jnp.dot(by_token, w_out, preferred_element_type=F32)
    residual = (residual_in.astype(F32) + projected).astype(BF16)
    values = residual.astype(F32)
    scale = lax.rsqrt(jnp.mean(values * values, axis=-1, keepdims=True) + NORM_EPS)
    normed = (values * scale * ffn_gain.astype(F32)).astype(BF16)
    normed_other = lax.ppermute(normed, "sp_2", swap_cores)

    columns_axes = ("sp_0", "sp_1")
    arrived, swapped = [], []
    for c, source in enumerate((normed, normed_other)):
        send = (plans[c][0].T[:, None, :] == slots[None, :, None]).astype(BF16)
        rows = jnp.dot(send.reshape(columns * cap, quarter), source, preferred_element_type=F32).astype(BF16)
        rows = lax.all_to_all(rows.reshape(columns, cap, width), columns_axes, 0, 0, tiled=True)
        rows = rows.reshape(columns * cap, width)
        arrived.append(rows)
        swapped.append(lax.ppermute(rows, core_tp, ROW_PAIRS))
    sums = []
    for c in range(2):
        mine = ffn(arrived[c], own, other, F32)
        theirs = ffn(swapped[c], own, other, BF16)
        back = lax.ppermute(theirs, core_tp, ROW_PAIRS)
        out = (mine + back.astype(F32)).astype(BF16)
        home = lax.all_to_all(out.reshape(columns, cap, width), columns_axes, 0, 0, tiled=True)
        home = home.reshape(columns * cap, width)
        lead, rest = blend(plans[c][0], plans[c][1], cap)
        sums.append(jnp.dot(jnp.concatenate([lead, rest], axis=1), jnp.concatenate([home, home]), preferred_element_type=F32))
    from_other = lax.ppermute(sums[1], "sp_2", swap_cores)
    return (residual.astype(F32) + (sums[0] + from_other)).astype(BF16)


def solution(mesh):
    torus = Mesh(mesh.devices.reshape(8, 4, 2, mesh.shape["tp"]), ("sp_0", "sp_1", "sp_2", "tp"))
    placed = (
        P(SP_TP, None), P(SP, "tp"), P(SP, "tp"), P(SP, "tp"), P(SP, "tp"), P(SP, "tp"),
        P(), P(), P(),
        P(SP, None), P(SP_TP, None),
        P(SP, None, "tp"), P(SP, None, "tp"), P(SP, "tp", None),
    )

    return jax.shard_map(on_device, mesh=torus, in_specs=placed, out_specs=P(SP_TP, None), check_vma=False)
```

```python
import jax
import jax.numpy as jnp
from jax import lax
from jax.experimental import pallas as pl
from jax.experimental.pallas import tpu as pltpu
from jax.sharding import Mesh
from jax.sharding import PartitionSpec as P


DK = 64
DV = 128
BLOCK = 64
SP = ("sp_0", "sp_1", "sp_2")
SP_TP = ("sp_0", "sp_1", "sp_2", "tp")
PLANE = ("sp_1", "sp_2")
DECAY_TEMP = 16.0
CLAMP_LIMIT = 7.0
SIGMOID_SLOPE = 1.702
NORM_EPS = 1e-06
F32 = jnp.float32
BF16 = jnp.bfloat16

ROW_PAIRS = [(c * 4 + y, c * 4 + ((y ^ 1) if c == 0 else 3 - y)) for c in range(2) for y in range(4)]
WEIGHT_PAIRS = [(c * 4 + y, c * 4 + ((3 - y) if c == 0 else (y ^ 1))) for c in range(2) for y in range(4)]


def dot(a, b, dims):
    return lax.dot_general(a, b, (dims, ((), ())), preferred_element_type=F32)


def split3(x):
    hi = x.astype(BF16)
    rest = x - hi.astype(F32)
    mid = rest.astype(BF16)
    return hi, mid, (rest - mid.astype(F32)).astype(BF16)


def head_mask(shape):
    return lax.broadcasted_iota(jnp.int32, shape, 1) < DK


def pick_heads(both):
    top, bottom = both[:DV], both[DV:]
    return jnp.where(head_mask(top.shape), top, bottom)


def stack_heads(x):
    zero = jnp.zeros_like(x)
    mask = head_mask(x.shape)
    return jnp.concatenate([jnp.where(mask, x, zero), jnp.where(mask, zero, x)], axis=0)


def store_state(out_ref, state_t, log_total):
    packed = jnp.concatenate(
        [
            state_t,
            *(part.astype(F32) for part in split3(log_total)),
            jnp.zeros((5, 2 * DK), F32),
        ],
        axis=0,
    ).astype(BF16)
    for copy in range(out_ref.shape[0]):
        out_ref[copy] = packed


def load_state(ref, k):
    item = ref[k].astype(F32)
    return item[:DV], item[DV : DV + 1] + item[DV + 1 : DV + 2] + item[DV + 2 : DV + 3]


def local_kernel(k_ref, v_ref, d_ref, state_ref, cum_ref):
    logit = d_ref[...]
    logdecay = (jnp.minimum(logit, 0.0) - jnp.log1p(jnp.exp(-jnp.abs(logit)))) / DECAY_TEMP
    rows = logdecay.shape[0]
    low = (
        lax.broadcasted_iota(jnp.int32, (rows, rows), 0)
        >= lax.broadcasted_iota(jnp.int32, (rows, rows), 1)
    ).astype(F32).astype(BF16)
    cum = sum(dot(low, part, ((1,), (0,))) for part in split3(logdecay))
    cum_ref[...] = cum
    end = cum[rows - 1 : rows]
    kdec = (k_ref[...].astype(F32) * jnp.exp(end - cum)).astype(BF16)
    state_t = pick_heads(dot(v_ref[...], kdec, ((0,), (0,))))
    store_state(state_ref, state_t, end)


def inner_kernel(cum_ref, q_ref, k_ref, v_ref, inner_ref, qdec_ref):
    rows = q_ref.shape[0]
    half = BLOCK // 2
    cum_all = cum_ref[...]
    q_all = q_ref[...].astype(F32) * (DK**-0.5)
    qdec_ref[...] = (q_all * jnp.exp(cum_all)).astype(BF16)
    row = lax.broadcasted_iota(jnp.int32, (BLOCK, 2 * DK), 0)
    t = lax.broadcasted_iota(jnp.int32, (2 * BLOCK, BLOCK), 0) % BLOCK
    s = lax.broadcasted_iota(jnp.int32, (2 * BLOCK, BLOCK), 1)
    near = (t >= s) & ((t < half) == (s < half))
    far = (t >= half) & (s < half)
    state = jnp.zeros((DV, 2 * DK), F32)
    for b in range(rows // BLOCK):
        at = slice(b * BLOCK, (b + 1) * BLOCK)
        cum = cum_all[at]
        if b:
            cum = cum - cum_all[b * BLOCK - 1 : b * BLOCK]
        q, k, v = q_all[at], k_ref[at, :].astype(F32), v_ref[at, :]
        middle = jnp.where(row < half, cum[half // 2 - 1 : half // 2], cum[half + half // 2 - 1 : half + half // 2])
        border = cum[half - 1 : half]
        end = cum[BLOCK - 1 : BLOCK]
        shifted = cum - middle
        q_near = (q * jnp.exp(shifted)).astype(BF16)
        k_near = (k * jnp.exp(-shifted)).astype(BF16)
        q_far = (q * jnp.exp(jnp.minimum(cum - border, 0.0))).astype(BF16)
        k_far = (k * jnp.exp(jnp.minimum(border - cum, 0.0))).astype(BF16)
        s_near = dot(stack_heads(q_near), k_near, ((1,), (1,)))
        s_far = dot(stack_heads(q_far), k_far, ((1,), (1,)))
        scores = jnp.where(near, s_near, jnp.where(far, s_far, 0.0)).astype(BF16)
        part0 = dot(scores[:BLOCK], v[:, :DV], ((1,), (0,)))
        part1 = dot(scores[BLOCK:], v[:, DV:], ((1,), (0,)))
        if b:
            read = dot(stack_heads((q * jnp.exp(cum)).astype(BF16)), state.astype(BF16), ((1,), (1,)))
            part0 = part0 + read[:BLOCK]
            part1 = part1 + read[BLOCK:]
        inner_ref[at, :DV] = part0
        inner_ref[at, DV:] = part1
        if (b + 1) * BLOCK < rows:
            kdec = (k * jnp.exp(end - cum)).astype(BF16)
            added = pick_heads(dot(v, kdec, ((0,), (0,))))
            state = added if b == 0 else state * jnp.exp(end) + added


def plane_kernel(at_ref, all_ref, total_ref, before_ref, logb_ref):
    place = at_ref[0]
    before = total = jnp.zeros((DV, 2 * DK), F32)
    log_before = log_total = jnp.zeros((1, 2 * DK), F32)
    for k in range(all_ref.shape[0]):
        state, log = load_state(all_ref, k)
        decay = jnp.exp(log)
        total = total * decay + state
        log_total = log_total + log
        before = jnp.where(k < place, before * decay + state, before)
        log_before = jnp.where(k < place, log_before + log, log_before)
    store_state(total_ref, total, log_total)
    before_ref[...] = before
    logb_ref[...] = jnp.broadcast_to(log_before, logb_ref.shape)


def finish_kernel(at_ref, before_ref, logb_ref, inner_ref, qdec_ref, gate_ref, gain_ref, all_ref, out_ref):
    place = at_ref[0]
    state = jnp.zeros((DV, 2 * DK), F32)
    for k in range(all_ref.shape[0]):
        added, log = load_state(all_ref, k)
        state = jnp.where(k < place, state * jnp.exp(log) + added, state)
    state = state * jnp.exp(logb_ref[0:1]) + before_ref[...]
    read = dot(stack_heads(qdec_ref[...]), state.astype(BF16), ((1,), (1,)))
    rows = inner_ref.shape[0]
    quarter = rows // out_ref.shape[0]
    gain = gain_ref[...].astype(F32)
    for h in range(2):
        cols = slice(h * DV, (h + 1) * DV)
        attended = inner_ref[:, cols] + read[h * rows : (h + 1) * rows]
        scale = lax.rsqrt(jnp.mean(attended * attended, axis=1, keepdims=True) + NORM_EPS)
        gate = gate_ref[:, cols].astype(F32)
        mixed = (attended * scale * gain * (gate / (1.0 + jnp.exp(-gate)))).astype(BF16)
        for j in range(out_ref.shape[0]):
            out_ref[j, :, cols] = mixed[j * quarter : (j + 1) * quarter]


SMALL = 16 * 2**20


def held(x):
    return pltpu.with_memory_space_constraint(x, pltpu.VMEM)


def call(kernel, outs, *args, kept=(), loads=(), scratch=(), flops=2**20, limit=None):
    specs = [
        pl.BlockSpec(memory_space=pltpu.SMEM if a.dtype == jnp.int32 else pltpu.VMEM) for a in args
    ]
    specs += [pl.BlockSpec(memory_space=pltpu.VMEM)] * len(kept)
    specs += [pl.BlockSpec(memory_space=pl.ANY)] * len(loads)
    return pl.pallas_call(
        kernel,
        out_shape=outs,
        in_specs=specs,
        out_specs=[pl.BlockSpec(memory_space=pltpu.VMEM)] * len(outs),
        scratch_shapes=scratch,
        cost_estimate=pl.CostEstimate(flops=flops, bytes_accessed=2**19, transcendentals=2**16),
        compiler_params=pltpu.CompilerParams(vmem_limit_bytes=limit),
    )(*args, *(held(a) for a in kept), *loads)


def shaped(shape, dtype):
    return jax.ShapeDtypeStruct(shape, dtype)


def resident(shape, dtype):
    return pltpu.VMEM(shape, dtype)


def mixer(queries, key_rows, value_rows, out_gate, decay_logit, head_gain):
    rows = queries.shape[0]
    planes, members, tps = lax.axis_size("sp_0"), lax.axis_size(PLANE), lax.axis_size("tp")
    packed = DV + 8
    state, cum = call(
        local_kernel,
        [shaped((members, packed, 2 * DK), BF16), shaped((rows, 2 * DK), F32)],
        key_rows, value_rows, decay_logit,
    )
    inner, qdec = call(
        inner_kernel,
        [resident((rows, 2 * DV), F32), resident((rows, 2 * DK), BF16)],
        cum, queries, key_rows, value_rows,
    )
    in_plane = lax.all_to_all(state, PLANE, 0, 0, tiled=True)
    total, before, logb = call(
        plane_kernel,
        [shaped((planes, packed, 2 * DK), BF16), shaped((DV, 2 * DK), F32), shaped((8, 2 * DK), F32)],
        lax.axis_index(PLANE)[None].astype(jnp.int32), kept=(in_plane,), limit=SMALL,
    )
    along = lax.all_to_all(total, "sp_0", 0, 0, tiled=True)
    (mixed,) = call(
        finish_kernel,
        [shaped((tps, rows // tps, 2 * DV), BF16)],
        lax.axis_index("sp_0")[None].astype(jnp.int32), before, logb, inner, qdec, out_gate,
        head_gain[None], kept=(along,), limit=SMALL,
    )
    return lax.all_to_all(mixed, "tp", 0, 0, tiled=True)


def clamped_unit(gate_pre, up_pre):
    gate_cut = jnp.minimum(gate_pre, CLAMP_LIMIT)
    up_cut = jnp.clip(up_pre, -CLAMP_LIMIT, CLAMP_LIMIT)
    return (up_cut + 1.0) * (gate_cut / (1.0 + jnp.exp(-SIGMOID_SLOPE * gate_cut)))


def ffn_kernel(x_ref, *refs):
    sources, out_ref, bufs, sem = refs[:-8], refs[-8], refs[-7:-1], refs[-1]
    copies, k = [], 0
    for buf in bufs:
        at, parts = 0, []
        while at < buf.shape[0]:
            rows = sources[k].shape[0]
            parts.append(pltpu.make_async_copy(sources[k], buf.at[pl.ds(at, rows)], sem.at[k]))
            at, k = at + rows, k + 1
        copies.append(parts)
    for parts in copies:
        for copy in parts:
            copy.start()

    def product(x, which):
        for copy in copies[which]:
            copy.wait()
        return dot(x, bufs[which][...], ((1,), (0,)))

    x = x_ref[...]
    total = None
    for half in (0, 3):
        gate_pre = product(x, half)
        up_pre = product(x, half + 1)
        part = product(clamped_unit(gate_pre, up_pre).astype(BF16), half + 2)
        total = part if total is None else total + part
    out_ref[...] = total.astype(out_ref.dtype)


def ffn(x, own, other, kind):
    rows, width = x.shape
    sources = (*own, *other)
    (out,) = call(
        ffn_kernel, [kind((rows, width), BF16)], x, loads=sources,
        scratch=[
            *(pltpu.VMEM(w.shape, w.dtype) for w in (*own, *own)),
            pltpu.SemaphoreType.DMA((len(sources),)),
        ],
        flops=12 * rows * width * own[0].shape[1],
    )
    return out


def prepare_kernel(res_ref, gain_ref, rank_ref, piece_ref, w_ref, residual_ref, normed_ref, rows_ref, buf, sem):
    count, _, wide = piece_ref.shape
    copies = [
        pltpu.make_async_copy(w_ref.at[pl.ds(j * wide, wide)], buf.at[j], sem.at[j]) for j in range(count)
    ]
    for copy in copies:
        copy.start()
    total = res_ref[...].astype(F32)
    for j in range(count):
        copies[j].wait()
        total = total + dot(piece_ref[j], buf[j], ((1,), (0,)))
    residual = total.astype(BF16)
    residual_ref[...] = residual
    values = residual.astype(F32)
    scale = lax.rsqrt(jnp.mean(values * values, axis=1, keepdims=True) + NORM_EPS)
    normed = (values * scale * gain_ref[...].astype(F32)).astype(BF16)
    normed_ref[...] = normed
    columns, cap, width = rows_ref.shape
    rank = rank_ref[...]
    slot = lax.broadcasted_iota(jnp.int32, (columns, cap, rank.shape[1]), 1).astype(F32)
    send = jnp.where(rank[:, None, :] == slot, 1.0, 0.0).reshape(columns * cap, rank.shape[1])
    rows = dot(send.astype(BF16), normed, ((1,), (0,))).astype(BF16)
    rows_ref[...] = rows.reshape(columns, cap, width)


def blend(rank, weight, cap):
    slots = jnp.arange(cap).astype(F32)
    full = jnp.where(rank[:, :, None] == slots, weight[:, :, None], 0.0).reshape(rank.shape[0], -1)
    lead = lax.reduce_precision(full, 8, 7)
    return lead.astype(BF16), (full - lead).astype(BF16)


def on_device(
    residual_in, queries, key_rows, value_rows, out_gate, decay_logit, head_gain, w_out, ffn_gain,
    routing, route_weight, w_gate, w_up, w_down,
):
    core_tp = ("sp_2", "tp")
    own = (w_gate[0], w_up[0], w_down[0])
    middle = w_up.shape[1] // 2
    other = []
    for w in (own[0], own[1][:middle], own[1][middle:], own[2]):
        other.append(lax.ppermute(w, core_tp, WEIGHT_PAIRS))
    experts, cores = lax.axis_size(SP), lax.axis_size("sp_2")
    columns = experts // cores
    quarter, width = residual_in.shape
    cap = 2 * routing.shape[0] * routing.shape[1] // (lax.axis_size("tp") * experts)
    slots = jnp.arange(cap).astype(F32)
    swap_cores = [(0, 1), (1, 0)]

    routes = lax.dynamic_slice_in_dim(routing, lax.axis_index("tp") * quarter, quarter, 0)
    named = routes[:, :, None] == jnp.arange(experts, dtype=jnp.int32)
    chosen = jnp.any(named, axis=1)
    weight = jnp.sum(jnp.where(named, route_weight[:, :, None], 0.0), axis=1)
    earlier = jnp.tril(jnp.ones((quarter, quarter), BF16), -1)
    rank = jnp.where(chosen, jnp.dot(earlier, chosen.astype(BF16), preferred_element_type=F32), -1.0)
    both = jnp.stack([rank, weight]).reshape(2, quarter, columns, cores)
    core = lax.axis_index("sp_2")
    here = lax.dynamic_index_in_dim(both, core, 3, keepdims=False)
    away = lax.dynamic_index_in_dim(both, 1 - core, 3, keepdims=False)
    theirs_plan = lax.ppermute(away, "sp_2", swap_cores)
    plans = (here, theirs_plan)

    pieces = mixer(queries, key_rows, value_rows, out_gate, decay_logit, head_gain)
    residual, normed, rows = call(
        prepare_kernel,
        [
            shaped((quarter, width), BF16),
            shaped((quarter, width), BF16),
            shaped((columns, cap, width), BF16),
        ],
        residual_in, ffn_gain[None], here[0].T, kept=(pieces,), loads=(w_out,),
        scratch=[
            pltpu.VMEM((pieces.shape[0], pieces.shape[2], width), BF16),
            pltpu.SemaphoreType.DMA((pieces.shape[0],)),
        ],
    )
    normed_other = lax.ppermute(normed, "sp_2", swap_cores)

    columns_axes = ("sp_0", "sp_1")
    arrived, swapped = [], []
    for c in range(2):
        if c:
            send = (theirs_plan[0].T[:, None, :] == slots[None, :, None]).astype(BF16)
            rows = jnp.dot(send.reshape(columns * cap, quarter), normed_other, preferred_element_type=F32)
            rows = rows.astype(BF16).reshape(columns, cap, width)
        rows = lax.all_to_all(rows, columns_axes, 0, 0, tiled=True)
        rows = rows.reshape(columns * cap, width)
        arrived.append(rows)
        swapped.append(lax.ppermute(rows, core_tp, ROW_PAIRS))
    sums = []
    for c in range(2):
        theirs = ffn(swapped[c], own, other, shaped)
        mine = ffn(arrived[c], own, other, resident)
        back = lax.ppermute(theirs, core_tp, ROW_PAIRS)
        out = (mine.astype(F32) + back.astype(F32)).astype(BF16)
        home = lax.all_to_all(out.reshape(columns, cap, width), columns_axes, 0, 0, tiled=True)
        home = home.reshape(columns * cap, width)
        lead, rest = blend(plans[c][0], plans[c][1], cap)
        sums.append(jnp.dot(jnp.concatenate([lead, rest], axis=1), jnp.concatenate([home, home]), preferred_element_type=F32))
    from_other = lax.ppermute(sums[1], "sp_2", swap_cores)
    return (residual.astype(F32) + (sums[0] + from_other)).astype(BF16)


def solution(mesh):
    torus = Mesh(mesh.devices.reshape(8, 4, 2, mesh.shape["tp"]), ("sp_0", "sp_1", "sp_2", "tp"))
    placed = (
        P(SP_TP, None), P(SP, "tp"), P(SP, "tp"), P(SP, "tp"), P(SP, "tp"), P(SP, "tp"),
        P(), P(), P(),
        P(SP, None), P(SP_TP, None),
        P(SP, None, "tp"), P(SP, None, "tp"), P(SP, "tp", None),
    )

    return jax.shard_map(on_device, mesh=torus, in_specs=placed, out_specs=P(SP_TP, None), check_vma=False)
```

```python
import jax
import jax.numpy as jnp
from jax import lax
from jax.experimental import pallas as pl
from jax.experimental.pallas import tpu as pltpu
from jax.sharding import Mesh
from jax.sharding import PartitionSpec as P


DK = 64
DV = 128
BLOCK = 64
SP = ("sp_0", "sp_1", "sp_2")
SP_TP = ("sp_0", "sp_1", "sp_2", "tp")
PLANE = ("sp_1", "sp_2")
DECAY_TEMP = 16.0
CLAMP_LIMIT = 7.0
SIGMOID_SLOPE = 1.702
NORM_EPS = 1e-06
F32 = jnp.float32
BF16 = jnp.bfloat16

ROW_PAIRS = [(c * 4 + y, c * 4 + ((y ^ 1) if c == 0 else 3 - y)) for c in range(2) for y in range(4)]
WEIGHT_PAIRS = [(c * 4 + y, c * 4 + ((3 - y) if c == 0 else (y ^ 1))) for c in range(2) for y in range(4)]


def dot(a, b, dims):
    return lax.dot_general(a, b, (dims, ((), ())), preferred_element_type=F32)


def split3(x):
    hi = x.astype(BF16)
    rest = x - hi.astype(F32)
    mid = rest.astype(BF16)
    return hi, mid, (rest - mid.astype(F32)).astype(BF16)


def head_mask(shape):
    return lax.broadcasted_iota(jnp.int32, shape, 1) < DK


def pick_heads(both):
    top, bottom = both[:DV], both[DV:]
    return jnp.where(head_mask(top.shape), top, bottom)


def stack_heads(x):
    zero = jnp.zeros_like(x)
    mask = head_mask(x.shape)
    return jnp.concatenate([jnp.where(mask, x, zero), jnp.where(mask, zero, x)], axis=0)


def store_state(out_ref, state_t, log_total):
    packed = jnp.concatenate(
        [
            state_t,
            *(part.astype(F32) for part in split3(log_total)),
            jnp.zeros((5, 2 * DK), F32),
        ],
        axis=0,
    ).astype(BF16)
    for copy in range(out_ref.shape[0]):
        out_ref[copy] = packed


def load_state(ref, k):
    item = ref[k].astype(F32)
    return item[:DV], item[DV : DV + 1] + item[DV + 1 : DV + 2] + item[DV + 2 : DV + 3]


def local_kernel(k_ref, v_ref, d_ref, state_ref, cum_ref):
    logit = d_ref[...]
    logdecay = (jnp.minimum(logit, 0.0) - jnp.log1p(jnp.exp(-jnp.abs(logit)))) / DECAY_TEMP
    rows = logdecay.shape[0]
    low = (
        lax.broadcasted_iota(jnp.int32, (rows, rows), 0)
        >= lax.broadcasted_iota(jnp.int32, (rows, rows), 1)
    ).astype(F32).astype(BF16)
    cum = sum(dot(low, part, ((1,), (0,))) for part in split3(logdecay))
    cum_ref[...] = cum
    end = cum[rows - 1 : rows]
    kdec = (k_ref[...].astype(F32) * jnp.exp(end - cum)).astype(BF16)
    state_t = pick_heads(dot(v_ref[...], kdec, ((0,), (0,))))
    store_state(state_ref, state_t, end)


def inner_kernel(cum_ref, q_ref, k_ref, v_ref, inner_ref, qdec_ref):
    rows = q_ref.shape[0]
    half = BLOCK // 2
    cum_all = cum_ref[...]
    q_all = q_ref[...].astype(F32) * (DK**-0.5)
    qdec_ref[...] = (q_all * jnp.exp(cum_all)).astype(BF16)
    row = lax.broadcasted_iota(jnp.int32, (BLOCK, 2 * DK), 0)
    t = lax.broadcasted_iota(jnp.int32, (2 * BLOCK, BLOCK), 0) % BLOCK
    s = lax.broadcasted_iota(jnp.int32, (2 * BLOCK, BLOCK), 1)
    near = (t >= s) & ((t < half) == (s < half))
    far = (t >= half) & (s < half)
    state = jnp.zeros((DV, 2 * DK), F32)
    for b in range(rows // BLOCK):
        at = slice(b * BLOCK, (b + 1) * BLOCK)
        cum = cum_all[at]
        if b:
            cum = cum - cum_all[b * BLOCK - 1 : b * BLOCK]
        q, k, v = q_all[at], k_ref[at, :].astype(F32), v_ref[at, :]
        middle = jnp.where(row < half, cum[half // 2 - 1 : half // 2], cum[half + half // 2 - 1 : half + half // 2])
        border = cum[half - 1 : half]
        end = cum[BLOCK - 1 : BLOCK]
        shifted = cum - middle
        q_near = (q * jnp.exp(shifted)).astype(BF16)
        k_near = (k * jnp.exp(-shifted)).astype(BF16)
        q_far = (q * jnp.exp(jnp.minimum(cum - border, 0.0))).astype(BF16)
        k_far = (k * jnp.exp(jnp.minimum(border - cum, 0.0))).astype(BF16)
        s_near = dot(stack_heads(q_near), k_near, ((1,), (1,)))
        s_far = dot(stack_heads(q_far), k_far, ((1,), (1,)))
        scores = jnp.where(near, s_near, jnp.where(far, s_far, 0.0)).astype(BF16)
        part0 = dot(scores[:BLOCK], v[:, :DV], ((1,), (0,)))
        part1 = dot(scores[BLOCK:], v[:, DV:], ((1,), (0,)))
        if b:
            read = dot(stack_heads((q * jnp.exp(cum)).astype(BF16)), state.astype(BF16), ((1,), (1,)))
            part0 = part0 + read[:BLOCK]
            part1 = part1 + read[BLOCK:]
        inner_ref[at, :DV] = part0
        inner_ref[at, DV:] = part1
        if (b + 1) * BLOCK < rows:
            kdec = (k * jnp.exp(end - cum)).astype(BF16)
            added = pick_heads(dot(v, kdec, ((0,), (0,))))
            state = added if b == 0 else state * jnp.exp(end) + added


def plane_kernel(at_ref, all_ref, total_ref, before_ref, logb_ref):
    place = at_ref[0]
    before = total = jnp.zeros((DV, 2 * DK), F32)
    log_before = log_total = jnp.zeros((1, 2 * DK), F32)
    for k in range(all_ref.shape[0]):
        state, log = load_state(all_ref, k)
        decay = jnp.exp(log)
        total = total * decay + state
        log_total = log_total + log
        before = jnp.where(k < place, before * decay + state, before)
        log_before = jnp.where(k < place, log_before + log, log_before)
    store_state(total_ref, total, log_total)
    before_ref[...] = before
    logb_ref[...] = jnp.broadcast_to(log_before, logb_ref.shape)


def finish_kernel(at_ref, before_ref, logb_ref, inner_ref, qdec_ref, gate_ref, gain_ref, all_ref, out_ref):
    place = at_ref[0]
    state = jnp.zeros((DV, 2 * DK), F32)
    for k in range(all_ref.shape[0]):
        added, log = load_state(all_ref, k)
        state = jnp.where(k < place, state * jnp.exp(log) + added, state)
    state = state * jnp.exp(logb_ref[0:1]) + before_ref[...]
    read = dot(stack_heads(qdec_ref[...]), state.astype(BF16), ((1,), (1,)))
    rows = inner_ref.shape[0]
    quarter = rows // out_ref.shape[0]
    gain = gain_ref[...].astype(F32)
    for h in range(2):
        cols = slice(h * DV, (h + 1) * DV)
        attended = inner_ref[:, cols] + read[h * rows : (h + 1) * rows]
        scale = lax.rsqrt(jnp.mean(attended * attended, axis=1, keepdims=True) + NORM_EPS)
        gate = gate_ref[:, cols].astype(F32)
        mixed = (attended * scale * gain * (gate / (1.0 + jnp.exp(-gate)))).astype(BF16)
        for j in range(out_ref.shape[0]):
            out_ref[j, :, cols] = mixed[j * quarter : (j + 1) * quarter]


SMALL = 16 * 2**20


def held(x):
    return pltpu.with_memory_space_constraint(x, pltpu.VMEM)


def call(kernel, outs, *args, kept=(), loads=(), scratch=(), flops=2**20, limit=None):
    specs = [
        pl.BlockSpec(memory_space=pltpu.SMEM if a.dtype == jnp.int32 else pltpu.VMEM) for a in args
    ]
    specs += [pl.BlockSpec(memory_space=pltpu.VMEM)] * len(kept)
    specs += [pl.BlockSpec(memory_space=pl.ANY)] * len(loads)
    return pl.pallas_call(
        kernel,
        out_shape=outs,
        in_specs=specs,
        out_specs=[pl.BlockSpec(memory_space=pltpu.VMEM)] * len(outs),
        scratch_shapes=scratch,
        cost_estimate=pl.CostEstimate(flops=flops, bytes_accessed=2**19, transcendentals=2**16),
        compiler_params=pltpu.CompilerParams(vmem_limit_bytes=limit),
    )(*args, *(held(a) for a in kept), *(pltpu.with_memory_space_constraint(a, pltpu.HBM) for a in loads))


def shaped(shape, dtype):
    return jax.ShapeDtypeStruct(shape, dtype)


def resident(shape, dtype):
    return pltpu.VMEM(shape, dtype)


def mixer(queries, key_rows, value_rows, out_gate, decay_logit, head_gain):
    rows = queries.shape[0]
    planes, members, tps = lax.axis_size("sp_0"), lax.axis_size(PLANE), lax.axis_size("tp")
    packed = DV + 8
    state, cum = call(
        local_kernel,
        [shaped((members, packed, 2 * DK), BF16), shaped((rows, 2 * DK), F32)],
        key_rows, value_rows, decay_logit,
    )
    inner, qdec = call(
        inner_kernel,
        [resident((rows, 2 * DV), F32), resident((rows, 2 * DK), BF16)],
        cum, queries, key_rows, value_rows,
    )
    in_plane = lax.all_to_all(state, PLANE, 0, 0, tiled=True)
    total, before, logb = call(
        plane_kernel,
        [shaped((planes, packed, 2 * DK), BF16), shaped((DV, 2 * DK), F32), shaped((8, 2 * DK), F32)],
        lax.axis_index(PLANE)[None].astype(jnp.int32), kept=(in_plane,), limit=SMALL,
    )
    along = lax.all_to_all(total, "sp_0", 0, 0, tiled=True)
    (mixed,) = call(
        finish_kernel,
        [shaped((tps, rows // tps, 2 * DV), BF16)],
        lax.axis_index("sp_0")[None].astype(jnp.int32), before, logb, inner, qdec, out_gate,
        head_gain[None], kept=(along,), limit=SMALL,
    )
    return lax.all_to_all(mixed, "tp", 0, 0, tiled=True)


def clamped_unit(gate_pre, up_pre):
    gate_cut = jnp.minimum(gate_pre, CLAMP_LIMIT)
    up_cut = jnp.clip(up_pre, -CLAMP_LIMIT, CLAMP_LIMIT)
    return (up_cut + 1.0) * (gate_cut / (1.0 + jnp.exp(-SIGMOID_SLOPE * gate_cut)))


def load_kernel(*refs):
    count = len(refs) // 2
    sources, targets, sem = refs[:count], refs[count:-1], refs[-1]
    copies = [pltpu.make_async_copy(a, b, sem.at[k]) for k, (a, b) in enumerate(zip(sources, targets))]
    for copy in copies:
        copy.start()
    for copy in copies:
        copy.wait()


def load(arrays):
    return call(
        load_kernel, [resident(a.shape, a.dtype) for a in arrays], loads=arrays,
        scratch=[pltpu.SemaphoreType.DMA((len(arrays),))], limit=SMALL,
    )


def expert_part(x, gate_cols, up_cols, down_rows):
    gate_pre = dot(x, gate_cols[...], ((1,), (0,)))
    up_pre = dot(x, up_cols[...], ((1,), (0,)))
    hidden = clamped_unit(gate_pre, up_pre).astype(BF16)
    return dot(hidden, down_rows[...], ((1,), (0,)))


def ffn_kernel(x_ref, g0, u0, d0, g1, u1, d1, out_ref):
    x = x_ref[...]
    out_ref[...] = (expert_part(x, g0, u0, d0) + expert_part(x, g1, u1, d1)).astype(out_ref.dtype)


def ffn(x, weights, kind):
    rows, width = x.shape
    (out,) = call(
        ffn_kernel, [kind((rows, width), BF16)], kept=(x, *weights), limit=SMALL,
        flops=12 * rows * width * weights[0].shape[1],
    )
    return out


def prepare_kernel(res_ref, gain_ref, rank_ref, piece_ref, w_ref, residual_ref, normed_ref, rows_ref, buf, sem):
    count, _, wide = piece_ref.shape
    copies = [
        pltpu.make_async_copy(w_ref.at[pl.ds(j * wide, wide)], buf.at[j], sem.at[j]) for j in range(count)
    ]
    for copy in copies:
        copy.start()
    total = res_ref[...].astype(F32)
    for j in range(count):
        copies[j].wait()
        total = total + dot(piece_ref[j], buf[j], ((1,), (0,)))
    residual = total.astype(BF16)
    residual_ref[...] = residual
    values = residual.astype(F32)
    scale = lax.rsqrt(jnp.mean(values * values, axis=1, keepdims=True) + NORM_EPS)
    normed = (values * scale * gain_ref[...].astype(F32)).astype(BF16)
    normed_ref[...] = normed
    columns, cap, width = rows_ref.shape
    rank = rank_ref[...]
    slot = lax.broadcasted_iota(jnp.int32, (columns, cap, rank.shape[1]), 1).astype(F32)
    send = jnp.where(rank[:, None, :] == slot, 1.0, 0.0).reshape(columns * cap, rank.shape[1])
    rows = dot(send.astype(BF16), normed, ((1,), (0,))).astype(BF16)
    rows_ref[...] = rows.reshape(columns, cap, width)


def blend(rank, weight, cap):
    slots = jnp.arange(cap).astype(F32)
    full = jnp.where(rank[:, :, None] == slots, weight[:, :, None], 0.0).reshape(rank.shape[0], -1)
    lead = lax.reduce_precision(full, 8, 7)
    return lead.astype(BF16), (full - lead).astype(BF16)


def on_device(
    residual_in, queries, key_rows, value_rows, out_gate, decay_logit, head_gain, w_out, ffn_gain,
    routing, route_weight, w_gate, w_up, w_down,
):
    core_tp = ("sp_2", "tp")
    own = (w_gate[0], w_up[0], w_down[0])
    other = []
    for w in own:
        other.append(lax.ppermute(w, core_tp, WEIGHT_PAIRS))
    experts, cores = lax.axis_size(SP), lax.axis_size("sp_2")
    columns = experts // cores
    quarter, width = residual_in.shape
    cap = 2 * routing.shape[0] * routing.shape[1] // (lax.axis_size("tp") * experts)
    slots = jnp.arange(cap).astype(F32)
    swap_cores = [(0, 1), (1, 0)]

    routes = lax.dynamic_slice_in_dim(routing, lax.axis_index("tp") * quarter, quarter, 0)
    named = routes[:, :, None] == jnp.arange(experts, dtype=jnp.int32)
    chosen = jnp.any(named, axis=1)
    weight = jnp.sum(jnp.where(named, route_weight[:, :, None], 0.0), axis=1)
    earlier = jnp.tril(jnp.ones((quarter, quarter), BF16), -1)
    rank = jnp.where(chosen, jnp.dot(earlier, chosen.astype(BF16), preferred_element_type=F32), -1.0)
    both = jnp.stack([rank, weight]).reshape(2, quarter, columns, cores)
    core = lax.axis_index("sp_2")
    here = lax.dynamic_index_in_dim(both, core, 3, keepdims=False)
    away = lax.dynamic_index_in_dim(both, 1 - core, 3, keepdims=False)
    theirs_plan = lax.ppermute(away, "sp_2", swap_cores)
    plans = (here, theirs_plan)

    pieces = mixer(queries, key_rows, value_rows, out_gate, decay_logit, head_gain)
    residual, normed, rows = call(
        prepare_kernel,
        [
            shaped((quarter, width), BF16),
            shaped((quarter, width), BF16),
            shaped((columns, cap, width), BF16),
        ],
        residual_in, ffn_gain[None], here[0].T, kept=(pieces,), loads=(w_out,),
        scratch=[
            pltpu.VMEM((pieces.shape[0], pieces.shape[2], width), BF16),
            pltpu.SemaphoreType.DMA((pieces.shape[0],)),
        ],
    )
    normed_other = lax.ppermute(normed, "sp_2", swap_cores)

    columns_axes = ("sp_0", "sp_1")
    arrived, swapped = [], []
    for c in range(2):
        if c:
            send = (theirs_plan[0].T[:, None, :] == slots[None, :, None]).astype(BF16)
            rows = jnp.dot(send.reshape(columns * cap, quarter), normed_other, preferred_element_type=F32)
            rows = rows.astype(BF16).reshape(columns, cap, width)
        rows = lax.all_to_all(rows, columns_axes, 0, 0, tiled=True)
        rows = rows.reshape(columns * cap, width)
        arrived.append(rows)
        swapped.append(lax.ppermute(rows, core_tp, ROW_PAIRS))
    sums = []
    for c in range(2):
        weights = load((*own, *other))
        theirs = ffn(swapped[c], weights, shaped)
        mine = ffn(arrived[c], weights, resident)
        back = lax.ppermute(theirs, core_tp, ROW_PAIRS)
        out = (mine.astype(F32) + back.astype(F32)).astype(BF16)
        home = lax.all_to_all(out.reshape(columns, cap, width), columns_axes, 0, 0, tiled=True)
        home = home.reshape(columns * cap, width)
        lead, rest = blend(plans[c][0], plans[c][1], cap)
        sums.append(jnp.dot(jnp.concatenate([lead, rest], axis=1), jnp.concatenate([home, home]), preferred_element_type=F32))
    from_other = lax.ppermute(sums[1], "sp_2", swap_cores)
    return (residual.astype(F32) + (sums[0] + from_other)).astype(BF16)


def solution(mesh):
    torus = Mesh(mesh.devices.reshape(8, 4, 2, mesh.shape["tp"]), ("sp_0", "sp_1", "sp_2", "tp"))
    placed = (
        P(SP_TP, None), P(SP, "tp"), P(SP, "tp"), P(SP, "tp"), P(SP, "tp"), P(SP, "tp"),
        P(), P(), P(),
        P(SP, None), P(SP_TP, None),
        P(SP, None, "tp"), P(SP, None, "tp"), P(SP, "tp", None),
    )

    return jax.shard_map(on_device, mesh=torus, in_specs=placed, out_specs=P(SP_TP, None), check_vma=False)
```

```python
import jax
import jax.numpy as jnp
from jax import lax
from jax.experimental import pallas as pl
from jax.experimental.pallas import tpu as pltpu
from jax.sharding import Mesh
from jax.sharding import PartitionSpec as P


DK = 64
DV = 128
BLOCK = 64
SP = ("sp_0", "sp_1", "sp_2")
SP_TP = ("sp_0", "sp_1", "sp_2", "tp")
PLANE = ("sp_1", "sp_2")
DECAY_TEMP = 16.0
CLAMP_LIMIT = 7.0
SIGMOID_SLOPE = 1.702
NORM_EPS = 1e-06
F32 = jnp.float32
BF16 = jnp.bfloat16

ROW_PAIRS = [(c * 4 + y, c * 4 + ((y ^ 1) if c == 0 else 3 - y)) for c in range(2) for y in range(4)]
CROSS_PAIRS = [(a, b ^ 4) for a, b in ROW_PAIRS]
WEIGHT_PAIRS = [(c * 4 + y, c * 4 + ((3 - y) if c == 0 else (y ^ 1))) for c in range(2) for y in range(4)]


def dot(a, b, dims):
    return lax.dot_general(a, b, (dims, ((), ())), preferred_element_type=F32)


def split3(x):
    hi = x.astype(BF16)
    rest = x - hi.astype(F32)
    mid = rest.astype(BF16)
    return hi, mid, (rest - mid.astype(F32)).astype(BF16)


def head_mask(shape):
    return lax.broadcasted_iota(jnp.int32, shape, 1) < DK


def pick_heads(both):
    top, bottom = both[:DV], both[DV:]
    return jnp.where(head_mask(top.shape), top, bottom)


def stack_heads(x):
    zero = jnp.zeros_like(x)
    mask = head_mask(x.shape)
    return jnp.concatenate([jnp.where(mask, x, zero), jnp.where(mask, zero, x)], axis=0)


def store_state(out_ref, state_t, log_total):
    packed = jnp.concatenate(
        [
            state_t,
            *(part.astype(F32) for part in split3(log_total)),
            jnp.zeros((5, 2 * DK), F32),
        ],
        axis=0,
    ).astype(BF16)
    for copy in range(out_ref.shape[0]):
        out_ref[copy] = packed


def load_state(ref, k):
    item = ref[k].astype(F32)
    return item[:DV], item[DV : DV + 1] + item[DV + 1 : DV + 2] + item[DV + 2 : DV + 3]


def local_kernel(k_ref, v_ref, d_ref, state_ref, cum_ref):
    logit = d_ref[...]
    logdecay = (jnp.minimum(logit, 0.0) - jnp.log1p(jnp.exp(-jnp.abs(logit)))) / DECAY_TEMP
    rows = logdecay.shape[0]
    low = (
        lax.broadcasted_iota(jnp.int32, (rows, rows), 0)
        >= lax.broadcasted_iota(jnp.int32, (rows, rows), 1)
    ).astype(F32).astype(BF16)
    cum = sum(dot(low, part, ((1,), (0,))) for part in split3(logdecay))
    cum_ref[...] = cum
    end = cum[rows - 1 : rows]
    kdec = (k_ref[...].astype(F32) * jnp.exp(end - cum)).astype(BF16)
    state_t = pick_heads(dot(v_ref[...], kdec, ((0,), (0,))))
    store_state(state_ref, state_t, end)


def inner_kernel(cum_ref, q_ref, k_ref, v_ref, inner_ref, qdec_ref):
    rows = q_ref.shape[0]
    half = BLOCK // 2
    cum_all = cum_ref[...]
    q_all = q_ref[...].astype(F32) * (DK**-0.5)
    qdec_ref[...] = (q_all * jnp.exp(cum_all)).astype(BF16)
    row = lax.broadcasted_iota(jnp.int32, (BLOCK, 2 * DK), 0)
    t = lax.broadcasted_iota(jnp.int32, (2 * BLOCK, BLOCK), 0) % BLOCK
    s = lax.broadcasted_iota(jnp.int32, (2 * BLOCK, BLOCK), 1)
    near = (t >= s) & ((t < half) == (s < half))
    far = (t >= half) & (s < half)
    state = jnp.zeros((DV, 2 * DK), F32)
    for b in range(rows // BLOCK):
        at = slice(b * BLOCK, (b + 1) * BLOCK)
        cum = cum_all[at]
        if b:
            cum = cum - cum_all[b * BLOCK - 1 : b * BLOCK]
        q, k, v = q_all[at], k_ref[at, :].astype(F32), v_ref[at, :]
        middle = jnp.where(row < half, cum[half // 2 - 1 : half // 2], cum[half + half // 2 - 1 : half + half // 2])
        border = cum[half - 1 : half]
        end = cum[BLOCK - 1 : BLOCK]
        shifted = cum - middle
        q_near = (q * jnp.exp(shifted)).astype(BF16)
        k_near = (k * jnp.exp(-shifted)).astype(BF16)
        q_far = (q * jnp.exp(jnp.minimum(cum - border, 0.0))).astype(BF16)
        k_far = (k * jnp.exp(jnp.minimum(border - cum, 0.0))).astype(BF16)
        s_near = dot(stack_heads(q_near), k_near, ((1,), (1,)))
        s_far = dot(stack_heads(q_far), k_far, ((1,), (1,)))
        scores = jnp.where(near, s_near, jnp.where(far, s_far, 0.0)).astype(BF16)
        part0 = dot(scores[:BLOCK], v[:, :DV], ((1,), (0,)))
        part1 = dot(scores[BLOCK:], v[:, DV:], ((1,), (0,)))
        if b:
            read = dot(stack_heads((q * jnp.exp(cum)).astype(BF16)), state.astype(BF16), ((1,), (1,)))
            part0 = part0 + read[:BLOCK]
            part1 = part1 + read[BLOCK:]
        inner_ref[at, :DV] = part0
        inner_ref[at, DV:] = part1
        if (b + 1) * BLOCK < rows:
            kdec = (k * jnp.exp(end - cum)).astype(BF16)
            added = pick_heads(dot(v, kdec, ((0,), (0,))))
            state = added if b == 0 else state * jnp.exp(end) + added


def plane_kernel(at_ref, all_ref, total_ref, before_ref, logb_ref):
    place = at_ref[0]
    before = total = jnp.zeros((DV, 2 * DK), F32)
    log_before = log_total = jnp.zeros((1, 2 * DK), F32)
    for k in range(all_ref.shape[0]):
        state, log = load_state(all_ref, k)
        decay = jnp.exp(log)
        total = total * decay + state
        log_total = log_total + log
        before = jnp.where(k < place, before * decay + state, before)
        log_before = jnp.where(k < place, log_before + log, log_before)
    store_state(total_ref, total, log_total)
    before_ref[...] = before
    logb_ref[...] = jnp.broadcast_to(log_before, logb_ref.shape)


def finish_kernel(at_ref, before_ref, logb_ref, inner_ref, qdec_ref, gate_ref, gain_ref, all_ref, out_ref):
    place = at_ref[0]
    state = jnp.zeros((DV, 2 * DK), F32)
    for k in range(all_ref.shape[0]):
        added, log = load_state(all_ref, k)
        state = jnp.where(k < place, state * jnp.exp(log) + added, state)
    state = state * jnp.exp(logb_ref[0:1]) + before_ref[...]
    read = dot(stack_heads(qdec_ref[...]), state.astype(BF16), ((1,), (1,)))
    rows = inner_ref.shape[0]
    quarter = rows // out_ref.shape[0]
    gain = gain_ref[...].astype(F32)
    for h in range(2):
        cols = slice(h * DV, (h + 1) * DV)
        attended = inner_ref[:, cols] + read[h * rows : (h + 1) * rows]
        scale = lax.rsqrt(jnp.mean(attended * attended, axis=1, keepdims=True) + NORM_EPS)
        gate = gate_ref[:, cols].astype(F32)
        mixed = (attended * scale * gain * (gate / (1.0 + jnp.exp(-gate)))).astype(BF16)
        for j in range(out_ref.shape[0]):
            out_ref[j, :, cols] = mixed[j * quarter : (j + 1) * quarter]


SMALL = 16 * 2**20


def held(x):
    return pltpu.with_memory_space_constraint(x, pltpu.VMEM)


def call(kernel, outs, *args, kept=(), loads=(), scratch=(), flops=2**20, limit=None):
    specs = [
        pl.BlockSpec(memory_space=pltpu.SMEM if a.dtype == jnp.int32 else pltpu.VMEM) for a in args
    ]
    specs += [pl.BlockSpec(memory_space=pltpu.VMEM)] * len(kept)
    specs += [pl.BlockSpec(memory_space=pl.ANY)] * len(loads)
    return pl.pallas_call(
        kernel,
        out_shape=outs,
        in_specs=specs,
        out_specs=[pl.BlockSpec(memory_space=pltpu.VMEM)] * len(outs),
        scratch_shapes=scratch,
        cost_estimate=pl.CostEstimate(flops=flops, bytes_accessed=2**19, transcendentals=2**16),
        compiler_params=pltpu.CompilerParams(vmem_limit_bytes=limit),
    )(*args, *(held(a) for a in kept), *(pltpu.with_memory_space_constraint(a, pltpu.HBM) for a in loads))


def shaped(shape, dtype):
    return jax.ShapeDtypeStruct(shape, dtype)


def resident(shape, dtype):
    return pltpu.VMEM(shape, dtype)


def mixer(queries, key_rows, value_rows, out_gate, decay_logit, head_gain):
    rows = queries.shape[0]
    planes, members, tps = lax.axis_size("sp_0"), lax.axis_size(PLANE), lax.axis_size("tp")
    packed = DV + 8
    state, cum = call(
        local_kernel,
        [shaped((members, packed, 2 * DK), BF16), shaped((rows, 2 * DK), F32)],
        key_rows, value_rows, decay_logit,
    )
    inner, qdec = call(
        inner_kernel,
        [resident((rows, 2 * DV), F32), resident((rows, 2 * DK), BF16)],
        cum, queries, key_rows, value_rows,
    )
    in_plane = lax.all_to_all(state, PLANE, 0, 0, tiled=True)
    total, before, logb = call(
        plane_kernel,
        [shaped((planes, packed, 2 * DK), BF16), shaped((DV, 2 * DK), F32), shaped((8, 2 * DK), F32)],
        lax.axis_index(PLANE)[None].astype(jnp.int32), kept=(in_plane,), limit=SMALL,
    )
    along = lax.all_to_all(total, "sp_0", 0, 0, tiled=True)
    (mixed,) = call(
        finish_kernel,
        [shaped((tps, rows // tps, 2 * DV), BF16)],
        lax.axis_index("sp_0")[None].astype(jnp.int32), before, logb, inner, qdec, out_gate,
        head_gain[None], kept=(along,), limit=SMALL,
    )
    return lax.all_to_all(mixed, "tp", 0, 0, tiled=True)


def clamped_unit(gate_pre, up_pre):
    gate_cut = jnp.minimum(gate_pre, CLAMP_LIMIT)
    up_cut = jnp.clip(up_pre, -CLAMP_LIMIT, CLAMP_LIMIT)
    return (up_cut + 1.0) * (gate_cut / (1.0 + jnp.exp(-SIGMOID_SLOPE * gate_cut)))


def load_kernel(*refs):
    count = len(refs) // 2
    sources, targets, sem = refs[:count], refs[count:-1], refs[-1]
    copies = [pltpu.make_async_copy(a, b, sem.at[k]) for k, (a, b) in enumerate(zip(sources, targets))]
    for copy in copies:
        copy.start()
    for copy in copies:
        copy.wait()


def load(arrays):
    return call(
        load_kernel, [resident(a.shape, a.dtype) for a in arrays], loads=arrays,
        scratch=[pltpu.SemaphoreType.DMA((len(arrays),))], limit=SMALL,
    )


def expert_part(x, gate_cols, up_cols, down_rows):
    gate_pre = dot(x, gate_cols[...], ((1,), (0,)))
    up_pre = dot(x, up_cols[...], ((1,), (0,)))
    hidden = clamped_unit(gate_pre, up_pre).astype(BF16)
    return dot(hidden, down_rows[...], ((1,), (0,)))


def ffn_kernel(x_ref, g0, u0, d0, g1, u1, d1, out_ref):
    x = x_ref[...]
    out_ref[...] = (expert_part(x, g0, u0, d0) + expert_part(x, g1, u1, d1)).astype(out_ref.dtype)


def ffn(x, weights, kind):
    rows, width = x.shape
    (out,) = call(
        ffn_kernel, [kind((rows, width), BF16)], kept=(x, *weights), limit=SMALL,
        flops=12 * rows * width * weights[0].shape[1],
    )
    return out


def prepare_kernel(res_ref, gain_ref, rank_ref, piece_ref, w_ref, residual_ref, normed_ref, rows_ref, buf, sem):
    count, _, wide = piece_ref.shape
    copies = [
        pltpu.make_async_copy(w_ref.at[pl.ds(j * wide, wide)], buf.at[j], sem.at[j]) for j in range(count)
    ]
    for copy in copies:
        copy.start()
    total = res_ref[...].astype(F32)
    for j in range(count):
        copies[j].wait()
        total = total + dot(piece_ref[j], buf[j], ((1,), (0,)))
    residual = total.astype(BF16)
    residual_ref[...] = residual
    values = residual.astype(F32)
    scale = lax.rsqrt(jnp.mean(values * values, axis=1, keepdims=True) + NORM_EPS)
    normed = (values * scale * gain_ref[...].astype(F32)).astype(BF16)
    normed_ref[...] = normed
    columns, cap, width = rows_ref.shape
    rank = rank_ref[...]
    slot = lax.broadcasted_iota(jnp.int32, (columns, cap, rank.shape[1]), 1).astype(F32)
    send = jnp.where(rank[:, None, :] == slot, 1.0, 0.0).reshape(columns * cap, rank.shape[1])
    rows = dot(send.astype(BF16), normed, ((1,), (0,))).astype(BF16)
    rows_ref[...] = rows.reshape(columns, cap, width)


def blend(rank, weight, cap):
    slots = jnp.arange(cap).astype(F32)
    full = jnp.where(rank[:, :, None] == slots, weight[:, :, None], 0.0).reshape(rank.shape[0], -1)
    lead = lax.reduce_precision(full, 8, 7)
    return lead.astype(BF16), (full - lead).astype(BF16)


def on_device(
    residual_in, queries, key_rows, value_rows, out_gate, decay_logit, head_gain, w_out, ffn_gain,
    routing, route_weight, w_gate, w_up, w_down,
):
    core_tp = ("sp_2", "tp")
    own = (w_gate[0], w_up[0], w_down[0])
    other = []
    for w in own:
        other.append(lax.ppermute(w, core_tp, WEIGHT_PAIRS))
    experts, cores = lax.axis_size(SP), lax.axis_size("sp_2")
    columns = experts // cores
    quarter, width = residual_in.shape
    cap = 2 * routing.shape[0] * routing.shape[1] // (lax.axis_size("tp") * experts)
    slots = jnp.arange(cap).astype(F32)
    swap_cores = [(0, 1), (1, 0)]

    routes = lax.dynamic_slice_in_dim(routing, lax.axis_index("tp") * quarter, quarter, 0)
    named = routes[:, :, None] == jnp.arange(experts, dtype=jnp.int32)
    chosen = jnp.any(named, axis=1)
    weight = jnp.sum(jnp.where(named, route_weight[:, :, None], 0.0), axis=1)
    earlier = jnp.tril(jnp.ones((quarter, quarter), BF16), -1)
    rank = jnp.where(chosen, jnp.dot(earlier, chosen.astype(BF16), preferred_element_type=F32), -1.0)
    both = jnp.stack([rank, weight]).reshape(2, quarter, columns, cores)
    core = lax.axis_index("sp_2")
    here = lax.dynamic_index_in_dim(both, core, 3, keepdims=False)
    away = lax.dynamic_index_in_dim(both, 1 - core, 3, keepdims=False)
    crossing = lax.ppermute(away[0], "sp_2", swap_cores)

    pieces = mixer(queries, key_rows, value_rows, out_gate, decay_logit, head_gain)
    residual, normed, rows = call(
        prepare_kernel,
        [
            shaped((quarter, width), BF16),
            shaped((quarter, width), BF16),
            shaped((columns, cap, width), BF16),
        ],
        residual_in, ffn_gain[None], here[0].T, kept=(pieces,), loads=(w_out,),
        scratch=[
            pltpu.VMEM((pieces.shape[0], pieces.shape[2], width), BF16),
            pltpu.SemaphoreType.DMA((pieces.shape[0],)),
        ],
    )
    normed_other = lax.ppermute(normed, "sp_2", swap_cores)

    columns_axes = ("sp_0", "sp_1")
    arrived, swapped = [], []
    for c in range(2):
        if c:
            send = (crossing.T[:, None, :] == slots[None, :, None]).astype(BF16)
            rows = jnp.dot(send.reshape(columns * cap, quarter), normed_other, preferred_element_type=F32)
            rows = rows.astype(BF16).reshape(columns, cap, width)
        rows = lax.all_to_all(rows, columns_axes, 0, 0, tiled=True)
        rows = rows.reshape(columns * cap, width)
        arrived.append(rows)
        swapped.append(lax.ppermute(rows, core_tp, ROW_PAIRS))
    routed = residual.astype(F32)
    for c, plan in enumerate((here, away)):
        weights = load((*own, *other))
        theirs = ffn(swapped[c], weights, shaped)
        mine = ffn(arrived[c], weights, resident)
        back = lax.ppermute(theirs, core_tp, CROSS_PAIRS if c else ROW_PAIRS)
        if c:
            mine = lax.ppermute(mine, "sp_2", swap_cores)
        out = (mine.astype(F32) + back.astype(F32)).astype(BF16)
        home = lax.all_to_all(out.reshape(columns, cap, width), columns_axes, 0, 0, tiled=True)
        home = home.reshape(columns * cap, width)
        parts = blend(plan[0], plan[1], cap)
        routed = routed + jnp.dot(
            jnp.concatenate(parts, axis=1), jnp.concatenate([home, home]), preferred_element_type=F32
        )
    return routed.astype(BF16)


def solution(mesh):
    torus = Mesh(mesh.devices.reshape(8, 4, 2, mesh.shape["tp"]), ("sp_0", "sp_1", "sp_2", "tp"))
    placed = (
        P(SP_TP, None), P(SP, "tp"), P(SP, "tp"), P(SP, "tp"), P(SP, "tp"), P(SP, "tp"),
        P(), P(), P(),
        P(SP, None), P(SP_TP, None),
        P(SP, None, "tp"), P(SP, None, "tp"), P(SP, "tp", None),
    )

    return jax.shard_map(on_device, mesh=torus, in_specs=placed, out_specs=P(SP_TP, None), check_vma=False)
```

```python
import jax
import jax.numpy as jnp
from jax import lax
from jax.experimental import pallas as pl
from jax.experimental.pallas import tpu as pltpu
from jax.sharding import Mesh
from jax.sharding import PartitionSpec as P


DK = 64
DV = 128
BLOCK = 64
SP = ("sp_0", "sp_1", "sp_2")
SP_TP = ("sp_0", "sp_1", "sp_2", "tp")
PLANE = ("sp_1", "sp_2")
DECAY_TEMP = 16.0
CLAMP_LIMIT = 7.0
SIGMOID_SLOPE = 1.702
NORM_EPS = 1e-06
F32 = jnp.float32
BF16 = jnp.bfloat16

ROW_PAIRS = [(c * 4 + y, c * 4 + ((y ^ 1) if c == 0 else 3 - y)) for c in range(2) for y in range(4)]
CROSS_PAIRS = [(a, b ^ 4) for a, b in ROW_PAIRS]
WEIGHT_PAIRS = [(c * 4 + y, c * 4 + ((3 - y) if c == 0 else (y ^ 1))) for c in range(2) for y in range(4)]


def dot(a, b, dims):
    return lax.dot_general(a, b, (dims, ((), ())), preferred_element_type=F32)


def split3(x):
    hi = x.astype(BF16)
    rest = x - hi.astype(F32)
    mid = rest.astype(BF16)
    return hi, mid, (rest - mid.astype(F32)).astype(BF16)


def head_mask(shape):
    return lax.broadcasted_iota(jnp.int32, shape, 1) < DK


def pick_heads(both):
    top, bottom = both[:DV], both[DV:]
    return jnp.where(head_mask(top.shape), top, bottom)


def stack_heads(x):
    zero = jnp.zeros_like(x)
    mask = head_mask(x.shape)
    return jnp.concatenate([jnp.where(mask, x, zero), jnp.where(mask, zero, x)], axis=0)


def store_state(out_ref, state_t, log_total):
    packed = jnp.concatenate(
        [
            state_t,
            *(part.astype(F32) for part in split3(log_total)),
            jnp.zeros((5, 2 * DK), F32),
        ],
        axis=0,
    ).astype(BF16)
    for copy in range(out_ref.shape[0]):
        out_ref[copy] = packed


def load_state(ref, k):
    item = ref[k].astype(F32)
    return item[:DV], item[DV : DV + 1] + item[DV + 1 : DV + 2] + item[DV + 2 : DV + 3]


def row_block(first, source, target, buf, sem):
    inward = pltpu.make_async_copy(source.at[pl.ds(first, buf.shape[0])], buf, sem.at[0])
    return inward, pltpu.make_async_copy(buf, target, sem.at[1])


def local_kernel(k_ref, v_ref, d_ref, w_ref, state_ref, cum_ref, part_ref, buf, sem):
    inward, outward = row_block(0, w_ref, part_ref, buf, sem)
    inward.start()
    logit = d_ref[...]
    logdecay = (jnp.minimum(logit, 0.0) - jnp.log1p(jnp.exp(-jnp.abs(logit)))) / DECAY_TEMP
    rows = logdecay.shape[0]
    low = (
        lax.broadcasted_iota(jnp.int32, (rows, rows), 0)
        >= lax.broadcasted_iota(jnp.int32, (rows, rows), 1)
    ).astype(F32).astype(BF16)
    cum = sum(dot(low, part, ((1,), (0,))) for part in split3(logdecay))
    cum_ref[...] = cum
    inward.wait()
    outward.start()
    end = cum[rows - 1 : rows]
    kdec = (k_ref[...].astype(F32) * jnp.exp(end - cum)).astype(BF16)
    state_t = pick_heads(dot(v_ref[...], kdec, ((0,), (0,))))
    store_state(state_ref, state_t, end)
    outward.wait()


def inner_kernel(cum_ref, q_ref, k_ref, v_ref, w_ref, inner_ref, qdec_ref, part_ref, buf, sem):
    inward, outward = row_block(buf.shape[0], w_ref, part_ref, buf, sem)
    inward.start()
    rows = q_ref.shape[0]
    half = BLOCK // 2
    cum_all = cum_ref[...]
    q_all = q_ref[...].astype(F32) * (DK**-0.5)
    qdec_ref[...] = (q_all * jnp.exp(cum_all)).astype(BF16)
    row = lax.broadcasted_iota(jnp.int32, (BLOCK, 2 * DK), 0)
    t = lax.broadcasted_iota(jnp.int32, (2 * BLOCK, BLOCK), 0) % BLOCK
    s = lax.broadcasted_iota(jnp.int32, (2 * BLOCK, BLOCK), 1)
    near = (t >= s) & ((t < half) == (s < half))
    far = (t >= half) & (s < half)
    state = jnp.zeros((DV, 2 * DK), F32)
    for b in range(rows // BLOCK):
        if b == 2:
            inward.wait()
            outward.start()
        at = slice(b * BLOCK, (b + 1) * BLOCK)
        cum = cum_all[at]
        if b:
            cum = cum - cum_all[b * BLOCK - 1 : b * BLOCK]
        q, k, v = q_all[at], k_ref[at, :].astype(F32), v_ref[at, :]
        middle = jnp.where(row < half, cum[half // 2 - 1 : half // 2], cum[half + half // 2 - 1 : half + half // 2])
        border = cum[half - 1 : half]
        end = cum[BLOCK - 1 : BLOCK]
        shifted = cum - middle
        q_near = (q * jnp.exp(shifted)).astype(BF16)
        k_near = (k * jnp.exp(-shifted)).astype(BF16)
        q_far = (q * jnp.exp(jnp.minimum(cum - border, 0.0))).astype(BF16)
        k_far = (k * jnp.exp(jnp.minimum(border - cum, 0.0))).astype(BF16)
        s_near = dot(stack_heads(q_near), k_near, ((1,), (1,)))
        s_far = dot(stack_heads(q_far), k_far, ((1,), (1,)))
        scores = jnp.where(near, s_near, jnp.where(far, s_far, 0.0)).astype(BF16)
        part0 = dot(scores[:BLOCK], v[:, :DV], ((1,), (0,)))
        part1 = dot(scores[BLOCK:], v[:, DV:], ((1,), (0,)))
        if b:
            read = dot(stack_heads((q * jnp.exp(cum)).astype(BF16)), state.astype(BF16), ((1,), (1,)))
            part0 = part0 + read[:BLOCK]
            part1 = part1 + read[BLOCK:]
        inner_ref[at, :DV] = part0
        inner_ref[at, DV:] = part1
        if (b + 1) * BLOCK < rows:
            kdec = (k * jnp.exp(end - cum)).astype(BF16)
            added = pick_heads(dot(v, kdec, ((0,), (0,))))
            state = added if b == 0 else state * jnp.exp(end) + added
    outward.wait()


def plane_kernel(at_ref, all_ref, total_ref, before_ref, logb_ref):
    place = at_ref[0]
    before = total = jnp.zeros((DV, 2 * DK), F32)
    log_before = log_total = jnp.zeros((1, 2 * DK), F32)
    for k in range(all_ref.shape[0]):
        state, log = load_state(all_ref, k)
        decay = jnp.exp(log)
        total = total * decay + state
        log_total = log_total + log
        before = jnp.where(k < place, before * decay + state, before)
        log_before = jnp.where(k < place, log_before + log, log_before)
    store_state(total_ref, total, log_total)
    before_ref[...] = before
    logb_ref[...] = jnp.broadcast_to(log_before, logb_ref.shape)


def finish_kernel(at_ref, before_ref, logb_ref, inner_ref, qdec_ref, gate_ref, gain_ref, all_ref, out_ref):
    place = at_ref[0]
    state = jnp.zeros((DV, 2 * DK), F32)
    for k in range(all_ref.shape[0]):
        added, log = load_state(all_ref, k)
        state = jnp.where(k < place, state * jnp.exp(log) + added, state)
    state = state * jnp.exp(logb_ref[0:1]) + before_ref[...]
    read = dot(stack_heads(qdec_ref[...]), state.astype(BF16), ((1,), (1,)))
    rows = inner_ref.shape[0]
    quarter = rows // out_ref.shape[0]
    gain = gain_ref[...].astype(F32)
    for h in range(2):
        cols = slice(h * DV, (h + 1) * DV)
        attended = inner_ref[:, cols] + read[h * rows : (h + 1) * rows]
        scale = lax.rsqrt(jnp.mean(attended * attended, axis=1, keepdims=True) + NORM_EPS)
        gate = gate_ref[:, cols].astype(F32)
        mixed = (attended * scale * gain * (gate / (1.0 + jnp.exp(-gate)))).astype(BF16)
        for j in range(out_ref.shape[0]):
            out_ref[j, :, cols] = mixed[j * quarter : (j + 1) * quarter]


SMALL = 16 * 2**20


def held(x):
    return pltpu.with_memory_space_constraint(x, pltpu.VMEM)


def call(kernel, outs, *args, kept=(), loads=(), scratch=(), flops=2**20, limit=None, parts=0):
    specs = [
        pl.BlockSpec(memory_space=pltpu.SMEM if a.dtype == jnp.int32 else pltpu.VMEM) for a in args
    ]
    specs += [pl.BlockSpec(memory_space=pltpu.VMEM)] * len(kept)
    specs += [pl.BlockSpec(memory_space=pl.ANY)] * len(loads)
    return pl.pallas_call(
        kernel,
        out_shape=outs,
        in_specs=specs,
        out_specs=[pl.BlockSpec(memory_space=pltpu.VMEM)] * (len(outs) - parts)
        + [pl.BlockSpec(memory_space=pl.ANY)] * parts,
        scratch_shapes=scratch,
        cost_estimate=pl.CostEstimate(flops=flops, bytes_accessed=2**19, transcendentals=2**16),
        compiler_params=pltpu.CompilerParams(vmem_limit_bytes=limit),
    )(*args, *(held(a) for a in kept), *(pltpu.with_memory_space_constraint(a, pltpu.HBM) for a in loads))


def shaped(shape, dtype):
    return jax.ShapeDtypeStruct(shape, dtype)


def resident(shape, dtype):
    return pltpu.VMEM(shape, dtype)


def mixer(queries, key_rows, value_rows, out_gate, decay_logit, head_gain, w_up):
    rows = queries.shape[0]
    half = shaped((w_up.shape[0] // 2, w_up.shape[1]), BF16)
    through = [pltpu.VMEM(half.shape, BF16), pltpu.SemaphoreType.DMA((2,))]
    planes, members, tps = lax.axis_size("sp_0"), lax.axis_size(PLANE), lax.axis_size("tp")
    packed = DV + 8
    state, cum, upper = call(
        local_kernel,
        [shaped((members, packed, 2 * DK), BF16), shaped((rows, 2 * DK), F32), half],
        key_rows, value_rows, decay_logit, loads=(w_up,), scratch=through, parts=1,
    )
    inner, qdec, lower = call(
        inner_kernel,
        [resident((rows, 2 * DV), F32), resident((rows, 2 * DK), BF16), half],
        cum, queries, key_rows, value_rows, loads=(w_up,), scratch=through, parts=1,
    )
    in_plane = lax.all_to_all(state, PLANE, 0, 0, tiled=True)
    total, before, logb = call(
        plane_kernel,
        [shaped((planes, packed, 2 * DK), BF16), shaped((DV, 2 * DK), F32), shaped((8, 2 * DK), F32)],
        lax.axis_index(PLANE)[None].astype(jnp.int32), kept=(in_plane,), limit=SMALL,
    )
    along = lax.all_to_all(total, "sp_0", 0, 0, tiled=True)
    (mixed,) = call(
        finish_kernel,
        [shaped((tps, rows // tps, 2 * DV), BF16)],
        lax.axis_index("sp_0")[None].astype(jnp.int32), before, logb, inner, qdec, out_gate,
        head_gain[None], kept=(along,), limit=SMALL,
    )
    return lax.all_to_all(mixed, "tp", 0, 0, tiled=True), upper, lower


def clamped_unit(gate_pre, up_pre):
    gate_cut = jnp.minimum(gate_pre, CLAMP_LIMIT)
    up_cut = jnp.clip(up_pre, -CLAMP_LIMIT, CLAMP_LIMIT)
    return (up_cut + 1.0) * (gate_cut / (1.0 + jnp.exp(-SIGMOID_SLOPE * gate_cut)))


def load_kernel(*refs):
    sources, targets, sem = list(refs[:7]), refs[7:13], refs[13]
    copies = []
    for target in targets:
        at = 0
        while at < target.shape[0]:
            source = sources.pop(0)
            place = target.at[pl.ds(at, source.shape[0])]
            copies.append(pltpu.make_async_copy(source, place, sem.at[len(copies)]))
            at += source.shape[0]
    for copy in copies:
        copy.start()
    for copy in copies:
        copy.wait()


def load(own, other):
    return call(
        load_kernel, [resident(a.shape, a.dtype) for a in (*own, *own)], loads=(*own, *other),
        scratch=[pltpu.SemaphoreType.DMA((7,))], limit=SMALL,
    )


def expert_part(x, gate_cols, up_cols, down_rows):
    gate_pre = dot(x, gate_cols[...], ((1,), (0,)))
    up_pre = dot(x, up_cols[...], ((1,), (0,)))
    hidden = clamped_unit(gate_pre, up_pre).astype(BF16)
    return dot(hidden, down_rows[...], ((1,), (0,)))


def ffn_kernel(x_ref, g0, u0, d0, g1, u1, d1, out_ref):
    x = x_ref[...]
    out_ref[...] = (expert_part(x, g0, u0, d0) + expert_part(x, g1, u1, d1)).astype(out_ref.dtype)


def ffn(x, weights, kind):
    rows, width = x.shape
    (out,) = call(
        ffn_kernel, [kind((rows, width), BF16)], kept=(x, *weights), limit=SMALL,
        flops=12 * rows * width * weights[0].shape[1],
    )
    return out


def prepare_kernel(res_ref, gain_ref, rank_ref, piece_ref, w_ref, residual_ref, normed_ref, rows_ref, buf, sem):
    count, _, wide = piece_ref.shape
    copies = [
        pltpu.make_async_copy(w_ref.at[pl.ds(j * wide, wide)], buf.at[j], sem.at[j]) for j in range(count)
    ]
    for copy in copies:
        copy.start()
    total = res_ref[...].astype(F32)
    for j in range(count):
        copies[j].wait()
        total = total + dot(piece_ref[j], buf[j], ((1,), (0,)))
    residual = total.astype(BF16)
    residual_ref[...] = residual
    values = residual.astype(F32)
    scale = lax.rsqrt(jnp.mean(values * values, axis=1, keepdims=True) + NORM_EPS)
    normed = (values * scale * gain_ref[...].astype(F32)).astype(BF16)
    normed_ref[...] = normed
    columns, cap, width = rows_ref.shape
    rank = rank_ref[...]
    slot = lax.broadcasted_iota(jnp.int32, (columns, cap, rank.shape[1]), 1).astype(F32)
    send = jnp.where(rank[:, None, :] == slot, 1.0, 0.0).reshape(columns * cap, rank.shape[1])
    rows = dot(send.astype(BF16), normed, ((1,), (0,))).astype(BF16)
    rows_ref[...] = rows.reshape(columns, cap, width)


def blend(rank, weight, cap):
    slots = jnp.arange(cap).astype(F32)
    full = jnp.where(rank[:, :, None] == slots, weight[:, :, None], 0.0).reshape(rank.shape[0], -1)
    lead = lax.reduce_precision(full, 8, 7)
    return lead.astype(BF16), (full - lead).astype(BF16)


def on_device(
    residual_in, queries, key_rows, value_rows, out_gate, decay_logit, head_gain, w_out, ffn_gain,
    routing, route_weight, w_gate, w_up, w_down,
):
    core_tp = ("sp_2", "tp")
    own = (w_gate[0], w_up[0], w_down[0])
    experts, cores = lax.axis_size(SP), lax.axis_size("sp_2")
    columns = experts // cores
    quarter, width = residual_in.shape
    cap = 2 * routing.shape[0] * routing.shape[1] // (lax.axis_size("tp") * experts)
    slots = jnp.arange(cap).astype(F32)
    swap_cores = [(0, 1), (1, 0)]

    routes = lax.dynamic_slice_in_dim(routing, lax.axis_index("tp") * quarter, quarter, 0)
    named = routes[:, :, None] == jnp.arange(experts, dtype=jnp.int32)
    chosen = jnp.any(named, axis=1)
    weight = jnp.sum(jnp.where(named, route_weight[:, :, None], 0.0), axis=1)
    earlier = jnp.tril(jnp.ones((quarter, quarter), BF16), -1)
    rank = jnp.where(chosen, jnp.dot(earlier, chosen.astype(BF16), preferred_element_type=F32), -1.0)
    both = jnp.stack([rank, weight]).reshape(2, quarter, columns, cores)
    core = lax.axis_index("sp_2")
    here = lax.dynamic_index_in_dim(both, core, 3, keepdims=False)
    away = lax.dynamic_index_in_dim(both, 1 - core, 3, keepdims=False)
    crossing = lax.ppermute(away[0], "sp_2", swap_cores)

    pieces, upper, lower = mixer(
        queries, key_rows, value_rows, out_gate, decay_logit, head_gain, own[1]
    )
    other = []
    for w in (own[0], upper, lower, own[2]):
        other.append(lax.ppermute(w, core_tp, WEIGHT_PAIRS))
    residual, normed, rows = call(
        prepare_kernel,
        [
            shaped((quarter, width), BF16),
            shaped((quarter, width), BF16),
            shaped((columns, cap, width), BF16),
        ],
        residual_in, ffn_gain[None], here[0].T, kept=(pieces,), loads=(w_out,),
        scratch=[
            pltpu.VMEM((pieces.shape[0], pieces.shape[2], width), BF16),
            pltpu.SemaphoreType.DMA((pieces.shape[0],)),
        ],
    )
    normed_other = lax.ppermute(normed, "sp_2", swap_cores)

    columns_axes = ("sp_0", "sp_1")
    arrived, swapped = [], []
    for c in range(2):
        if c:
            send = (crossing.T[:, None, :] == slots[None, :, None]).astype(BF16)
            rows = jnp.dot(send.reshape(columns * cap, quarter), normed_other, preferred_element_type=F32)
            rows = rows.astype(BF16).reshape(columns, cap, width)
        rows = lax.all_to_all(rows, columns_axes, 0, 0, tiled=True)
        rows = rows.reshape(columns * cap, width)
        arrived.append(rows)
        swapped.append(lax.ppermute(rows, core_tp, ROW_PAIRS))
    routed = residual.astype(F32)
    for c, plan in enumerate((here, away)):
        weights = load(own, other)
        theirs = ffn(swapped[c], weights, shaped)
        mine = ffn(arrived[c], weights, resident)
        back = lax.ppermute(theirs, core_tp, CROSS_PAIRS if c else ROW_PAIRS)
        if c:
            mine = lax.ppermute(mine, "sp_2", swap_cores)
        out = (mine.astype(F32) + back.astype(F32)).astype(BF16)
        home = lax.all_to_all(out.reshape(columns, cap, width), columns_axes, 0, 0, tiled=True)
        home = home.reshape(columns * cap, width)
        parts = blend(plan[0], plan[1], cap)
        routed = routed + jnp.dot(
            jnp.concatenate(parts, axis=1), jnp.concatenate([home, home]), preferred_element_type=F32
        )
    return routed.astype(BF16)


def solution(mesh):
    torus = Mesh(mesh.devices.reshape(8, 4, 2, mesh.shape["tp"]), ("sp_0", "sp_1", "sp_2", "tp"))
    placed = (
        P(SP_TP, None), P(SP, "tp"), P(SP, "tp"), P(SP, "tp"), P(SP, "tp"), P(SP, "tp"),
        P(), P(), P(),
        P(SP, None), P(SP_TP, None),
        P(SP, None, "tp"), P(SP, None, "tp"), P(SP, "tp", None),
    )

    return jax.shard_map(on_device, mesh=torus, in_specs=placed, out_specs=P(SP_TP, None), check_vma=False)
```
